32 devices in a mesh: grp: 2 (over x), ep: 16 (over z, y, core).
Axes of the slice: x: 2, y: 2, z: 4, core: 2. Of those that a mesh axis runs over, the one named last changes fastest.
Arguments:
- stream: bfloat16 [8192, 2048], P(('grp', 'ep')), parts along dimension 0, may hold values from -6 to 6
- norm_gain: float32 [2048], replicated, may hold values from 0.1 to 1.9
- routing: int32 [8192, 4], P(('grp', 'ep')), parts along dimension 0, may hold values from 0 to 31, all different within a row; in each aligned block of 256 rows (0 to 255, 256 to 511, ...) at most 64 rows name the same one
- gates: float32 [8192, 4], P(('grp', 'ep')), parts along dimension 0, may hold values from 0.1 to 1
- w_gate: bfloat16 [32, 2048, 512], P('ep'), may hold values from -0.125 to 0.125
- w_up: bfloat16 [32, 2048, 512], P('ep'), may hold values from -0.125 to 0.125
- w_down: bfloat16 [32, 512, 2048], P('ep'), may hold values from -0.25 to 0.25
- shared_gate: bfloat16 [2048, 512], replicated, may hold values from -0.125 to 0.125
- shared_up: bfloat16 [2048, 512], replicated, may hold values from -0.125 to 0.125
- shared_down: bfloat16 [512, 2048], replicated, may hold values from -0.25 to 0.25
Outputs:
- mixed: bfloat16 [8192, 2048], P(('grp', 'ep')), parts along dimension 0
The draws below stay inside these ranges and needn't reach their ends.
There are 2 independent parts, one for each index of `grp`. The reference program is written for one: setup_inputs(seed, part) draws one part's arguments, and reference() takes and returns one part's arrays. A program takes and returns all parts, laid end to end along the dimension named above; an argument that names none is the same for every part. Nothing has to cross between parts.
Inputs may be any that keep to these rules, and one draw needn't show every extreme that they name: `routing`: each token names 4 different experts. Among the 256 tokens of one index of ep no expert is named more than 64 times, and on some index an expert is named exactly 64 times.
All inputs are finite; a program needn't handle non-finite values.
Results may differ from the reference program's by a relative error of at most 0.007.
Values may be sent and summed in bfloat16 or wider, within the bound.
A program may use at most 128 MiB of HBM per device.

```python
import math
import jax
import jax.numpy as jnp
import numpy as np
from jax import lax

D = 2048
DE = 512
DS = 512
TOP_K = 4
TOK_DEV = 256
TOKENS = 4096
EXPERTS = 32
CAP = 64
N_EP = 16


def block_scale(stream_key, shape, split, low, high):
    level, own = 1.0, jax.random.fold_in(stream_key, 6)
    for axis_at, blocks in split:
        draws = jnp.exp(jax.random.uniform(jax.random.fold_in(own, axis_at), (blocks,), jnp.float32, low / len(split), high / len(split)))
        level = level * jnp.repeat(draws, shape[axis_at] // blocks).reshape([-1 if axis == axis_at else 1 for axis in range(len(shape))])
    return level


def deal_out(rng, own, number, rows, count, top, most, skew):
    sequence = jax.random.permutation(rng, count)
    packed, ordinary = load_shares(count, rows * top, most, skew, True), load_shares(count, rows * top, most, skew, False)
    places = jnp.arange(count)

    def named(sizes, offset_by):
        used = int((sizes > 0).sum())
        fixed = max(1, used // 4)
        moved = fixed + (places - fixed + offset_by * (used - fixed)) % max(1, count - fixed)
        return jnp.zeros((count,), jnp.int32).at[sequence[jnp.where(places < fixed, places, moved)]].set(jnp.asarray(sizes, jnp.int32))

    sizes = jnp.where(number % 4 == 0, named(packed, number // 4), named(ordinary, number - number // 4 - 1))
    mixed = jax.random.permutation(jax.random.fold_in(own, 3), count)
    donor, sink = mixed[0:count // 2 * 2:2], mixed[1:count // 2 * 2:2]
    slack = jnp.minimum(sizes[donor] - 1, most - sizes[sink]) // 2
    slack = jnp.where((donor == sequence[0]) | (sink == sequence[0]) | (sizes[sink] == 0), 0, jnp.maximum(slack, 0))
    moved = jax.random.randint(jax.random.fold_in(own, 4), (count // 2,), 0, 1 << 20) % (slack + 1)
    sizes = sizes.at[donor].add(-moved).at[sink].add(moved)
    members = jnp.searchsorted(jnp.cumsum(sizes), jnp.arange(rows * top), side="right").astype(jnp.int32)
    table = members.reshape(top, rows).T
    table = table[jax.random.permutation(jax.random.fold_in(own, 1), rows)]
    offset_by = jax.random.randint(jax.random.fold_in(own, 2), (rows, 1), 0, top)
    return jnp.take_along_axis(table, (jnp.arange(top)[None, :] + offset_by) % top, axis=1)


def load_shares(number_of, total, limit, slope, full):
    weights = [(1 << 20) // math.isqrt(standing ** slope) + 1 for standing in range(1, number_of + 1)]
    largest = limit if full else min(limit, max(-(-total // number_of), total * weights[0] // sum(weights)))
    least = 1 if total - largest >= number_of - 1 else 0
    counts, surplus = [largest] + [least] * (number_of - 1), total - largest - least * (number_of - 1)
    while surplus > 0:
        movable = [i for i in range(1, number_of) if counts[i] < largest] or [i for i in range(1, number_of) if counts[i] < limit]
        pool, left = sum([weights[i] for i in movable]), surplus
        for i in movable:
            extra = min(limit - counts[i], max(1, left * weights[i] // pool), surplus)
            counts[i] = counts[i] + extra
            surplus = surplus - extra
    return np.array(counts)


def gaussian(own_key, shape, spread, limit, pieces=(), kind=jnp.bfloat16):
    level = block_scale(own_key, shape, pieces, -0.22, 0.18) if pieces else 1.0
    entries = jax.random.normal(own_key, shape, jnp.float32) * spread * level
    return jnp.minimum(jnp.maximum(entries, -limit), limit).astype(kind)


def setup_inputs(seed: int = 0, part: int = 0) -> dict:
    streams_of = jax.random.split(jax.random.key(seed), 11)
    own_keys = jax.random.split(jax.random.fold_in(streams_of[10], part), 11)
    stream = gaussian(own_keys[0], (TOKENS, D), 1.0, 6.0, ((0, 16),))
    norm_gain = jnp.clip(1.0 + 0.18 * jax.random.normal(streams_of[1], (D,), jnp.float32), 0.1, 1.9)
    routing_keys = jax.random.split(jax.random.fold_in(own_keys[2], 1), TOKENS // TOK_DEV)
    routing_turns = jax.random.permutation(jax.random.fold_in(own_keys[2], 3), TOKENS // TOK_DEV)
    routing = jax.vmap(lambda own, number: deal_out(jax.random.fold_in(own_keys[2], 2), own, number, TOK_DEV, EXPERTS, TOP_K, CAP, 2))(routing_keys, routing_turns).reshape((TOKENS, TOP_K))
    gates = jnp.clip(0.1 + 0.9 * jax.random.uniform(own_keys[3], (TOKENS, TOP_K), jnp.float32) ** block_scale(own_keys[3], (TOKENS, TOP_K), ((0, 16),), -0.2, 0.2), 0.1, 1.0)
    w_gate = gaussian(streams_of[4], (EXPERTS, D, DE), D ** -0.5, 0.125, ((0, 16),))
    w_up = gaussian(streams_of[5], (EXPERTS, D, DE), D ** -0.5, 0.125, ((0, 16),))
    w_down = gaussian(streams_of[6], (EXPERTS, DE, D), DE ** -0.5, 0.25, ((0, 16),))
    shared_gate = gaussian(streams_of[7], (D, DS), D ** -0.5, 0.125)
    shared_up = gaussian(streams_of[8], (D, DS), D ** -0.5, 0.125)
    shared_down = gaussian(streams_of[9], (DS, D), DS ** -0.5, 0.25)
    return {"stream": stream, "norm_gain": norm_gain, "routing": routing, "gates": gates, "w_gate": w_gate, "w_up": w_up, "w_down": w_down, "shared_gate": shared_gate, "shared_up": shared_up, "shared_down": shared_down}


def layer_norm(stream, norm_gain):
    widened = stream.astype(jnp.float32)
    row_mean = lax.optimization_barrier(jnp.mean(widened, axis=-1, keepdims=True))
    variance = lax.optimization_barrier(jnp.mean(jnp.square(widened - row_mean), axis=-1, keepdims=True))
    return ((widened - row_mean) * lax.rsqrt(variance + 1e-05) * norm_gain).astype(jnp.bfloat16)

def reference(stream, norm_gain, routing, gates, w_gate, w_up, w_down, shared_gate, shared_up, shared_down):
    normed = layer_norm(stream, norm_gain)
    flat_ids = routing.reshape(-1)
    weights = gates.reshape(-1)
    total_rows = TOKENS * TOP_K
    capacity = N_EP * CAP

    def visit_expert(running, expert):
        chosen = jnp.nonzero(flat_ids == expert, size=capacity, fill_value=total_rows)[0].astype(jnp.int32)
        usable = chosen < total_rows
        clipped = jnp.minimum(chosen, total_rows - 1)
        token_ids = clipped // TOP_K
        gathered = normed[token_ids]
        gate_act = jnp.dot(gathered, w_gate[expert], preferred_element_type=jnp.float32)
        up_act = jnp.dot(gathered, w_up[expert], preferred_element_type=jnp.float32)
        hidden = (jax.nn.silu(gate_act) * up_act).astype(jnp.bfloat16)
        produced = jnp.dot(hidden, w_down[expert], preferred_element_type=jnp.float32).astype(jnp.bfloat16)
        weight_col = jnp.where(usable, weights[clipped], jnp.float32(0.0))
        running = running.at[token_ids].add(produced.astype(jnp.float32) * weight_col[:, None])
        return (running, None)
    start = jnp.zeros((TOKENS, D), jnp.float32)
    routed, _ = lax.scan(visit_expert, start, jnp.arange(EXPERTS, dtype=jnp.int32))
    shared_hidden = (jax.nn.silu(jnp.dot(normed, shared_gate, preferred_element_type=jnp.float32)) * jnp.dot(normed, shared_up, preferred_element_type=jnp.float32)).astype(jnp.bfloat16)
    shared_out = jnp.dot(shared_hidden, shared_down, preferred_element_type=jnp.float32)
    return (routed + shared_out).astype(jnp.bfloat16)
```

```python
import functools
import jax
import jax.numpy as jnp
from jax import lax
from jax.experimental import pallas as pl
from jax.experimental.pallas import tpu as pltpu
from jax.sharding import PartitionSpec as P


def layer_norm(stream, norm_gain):
    widened = stream.astype(jnp.float32)
    row_mean = jnp.mean(widened, axis=-1, keepdims=True)
    variance = jnp.mean(jnp.square(widened - row_mean), axis=-1, keepdims=True)
    return ((widened - row_mean) * lax.rsqrt(variance + 1e-05) * norm_gain).astype(jnp.bfloat16)


def shared_branch(normed, shared_gate, shared_up, shared_down):
    shared_hidden = (
        jax.nn.silu(jnp.dot(normed, shared_gate, preferred_element_type=jnp.float32))
        * jnp.dot(normed, shared_up, preferred_element_type=jnp.float32)
    ).astype(jnp.bfloat16)
    return jnp.dot(shared_hidden, shared_down, preferred_element_type=jnp.float32)


def serve_rows(received, w_gate, w_up, w_down):
    local_count = w_gate.shape[0]
    blocks = received.reshape((-1, local_count) + received.shape[1:])
    gate_act = jnp.einsum("sxcd,xdh->sxch", blocks, w_gate, preferred_element_type=jnp.float32)
    up_act = jnp.einsum("sxcd,xdh->sxch", blocks, w_up, preferred_element_type=jnp.float32)
    hidden = (jax.nn.silu(gate_act) * up_act).astype(jnp.bfloat16)
    produced = jnp.einsum(
        "sxch,xhd->sxcd", hidden, w_down, preferred_element_type=jnp.float32
    ).astype(jnp.bfloat16)
    return lax.all_to_all(
        produced.reshape(received.shape), "ep", split_axis=0, concat_axis=0, tiled=True
    )


def generic_device(
    stream, norm_gain, routing, gates, w_gate, w_up, w_down, shared_gate, shared_up, shared_down
):
    tok_rows, top_count = routing.shape
    local_count = w_gate.shape[0]
    peer_count = lax.axis_size("ep")
    experts = local_count * peer_count
    capacity = 2 * tok_rows * top_count // experts
    normed = layer_norm(stream, norm_gain)
    row_ids = jnp.arange(tok_rows, dtype=jnp.int32)
    lower = (row_ids[:, None] > row_ids[None, :]).astype(jnp.bfloat16)
    slot_ids = jnp.arange(capacity, dtype=jnp.int32).astype(jnp.float32)
    expert_hits = (
        routing[:, :, None] == jnp.arange(experts, dtype=jnp.int32)[None, None, :]
    ).astype(jnp.float32)
    token_hits = jnp.sum(expert_hits, axis=1).astype(jnp.bfloat16)
    earlier = jnp.dot(lower, token_hits, preferred_element_type=jnp.float32)
    slot_index = jnp.sum(earlier[:, None, :] * expert_hits, axis=2)
    slot_hits = (slot_index[:, :, None] == slot_ids[None, None, :]).astype(jnp.float32)
    gate_table = jnp.sum(
        gates[:, :, None, None] * expert_hits[:, :, :, None] * slot_hits[:, :, None, :], axis=1
    )
    all_normed = lax.all_gather(normed, "ep", axis=0, tiled=True)
    all_routing = lax.all_gather(routing, "ep", axis=0, tiled=True)
    first_expert = lax.axis_index("ep") * local_count
    shifted = all_routing.reshape(peer_count, tok_rows, top_count) - first_expert
    local_hits = (
        shifted[:, :, :, None] == jnp.arange(local_count, dtype=jnp.int32)[None, None, None, :]
    ).astype(jnp.float32)
    hits_here = jnp.sum(local_hits, axis=2).astype(jnp.bfloat16)
    prior_here = jnp.einsum("ab,pbx->pax", lower, hits_here, preferred_element_type=jnp.float32)
    placing_here = (
        hits_here.astype(jnp.float32)[:, :, :, None]
        * (prior_here[:, :, :, None] == slot_ids[None, None, None, :]).astype(jnp.float32)
    ).astype(jnp.bfloat16)
    sources = all_normed.reshape(peer_count, tok_rows, all_normed.shape[1])
    incoming = jnp.einsum(
        "ptxc,ptd->pxcd", placing_here, sources, preferred_element_type=jnp.float32
    ).astype(jnp.bfloat16)
    returned = serve_rows(
        incoming.reshape(peer_count * local_count, capacity, all_normed.shape[1]),
        w_gate,
        w_up,
        w_down,
    )
    weight_high = gate_table.astype(jnp.bfloat16)
    weight_low = (gate_table - weight_high.astype(jnp.float32)).astype(jnp.bfloat16)
    routed = jnp.einsum("tec,ecd->td", weight_high, returned, preferred_element_type=jnp.float32)
    routed = routed + jnp.einsum(
        "tec,ecd->td", weight_low, returned, preferred_element_type=jnp.float32
    )
    shared = shared_branch(normed, shared_gate, shared_up, shared_down)
    return (routed + shared).astype(jnp.bfloat16)


CORNER = (
    "gBA0", "gCA1", "gCA2", "gBA1", "gCA3", "xA", "gBC3", "gBA2", "gCB0", "gCB1", "gBC0", "gBC2",
    "gBA3", "gCB2", "xC", "sC", "sA", "rCC1", "gBG1", "gCD2", "xD", "sD", "gBG2", "xB",
    "rCD1", "rBD3", "rBD0", "xH", "sH", "rCC3", "rBH2", "rCH3", "rBH1", "rCH0", "xG", "sG",
    "sB", "gBF3", "rCG0", "gBE0", "rCG1", "rCG3", "rCG2", "rCC0", "gBE1", "rBB3", "xE", "sE",
    "xF", "sF", "rBE3", "rCF2", "rBF1", "rBB2", "rBF0", "rBD2", "rCF3", "rCE1", "rCE2", "fA2",
    "rBB0", "rBB1", "rCE0", "rCC2", "fA0", "fA3", "fA1",
)
MIDDLE = (
    "xC", "gAC3", "gDC3", "gEC3", "gEC1", "gDC0", "gAC2", "gAC0", "gDC1", "gAC1", "sC", "gED3",
    "gEA1", "gDE1", "gEA2", "gAD1", "gDA3", "gDB0", "gAG1", "gEB0", "gAG2", "gEB3", "gEB1", "gDH0",
    "gAH0", "gEB2", "gEC0", "gEC2", "xB", "xA", "sB", "gDH3", "gAH3", "gAG0", "xD", "gAG3",
    "gAF3", "xG", "sG", "sD", "gDE0", "gAE0", "gAE1", "xH", "gDE2", "gAE2", "xE", "sE",
    "sA", "sH", "rEE3", "gAF2", "rAD2", "xF", "sF", "rEH1", "rDA0", "rEH2", "rDF1", "rDG0",
    "rEG1", "rAB1", "rDG3", "rDD1", "rDF0", "rAB2", "rEG2", "rAA1", "rEH0", "rEH3", "rAA2", "rDF2",
    "rAB0", "rEF3", "rDB3", "rEE1", "rDD3", "rDD0", "rEE2", "rAA3", "fC1", "rEE0", "fC3", "fC2",
    "fC0",
)

PLANS = {"A": CORNER, "C": MIDDLE}
PARTS = 4


def across(block):
    return chr(65 + ((ord(block) - 65) ^ 1))


def ahead(block):
    n = ord(block) - 65
    return chr(65 + (3 - n // 2) * 2 + n % 2)


def seen_from(role, to, block):
    if to in ("A", "C"):
        return to, block
    if to in ("B", "D"):
        return role, across(block)
    return role, ahead(block)


SLOT = {role: {s[1]: i for i, s in enumerate([s for s in plan if s[0] == "s"])} for role, plan in PLANS.items()}
LANDING = {"A": {}, "C": {}}
for _role, _plan in PLANS.items():
    for _step in _plan:
        if _step[0] == "r":
            _there, _name = seen_from(_role, _step[1], _step[2])
            LANDING[_there][(_name, _step[3], _role, _step[1])] = len(LANDING[_there])
LANDINGS = max(len(v) for v in LANDING.values())
SENDS = 24 + max(sum(2 if s[0] == "g" else 1 for s in plan) for plan in PLANS.values())
R_META, R_SIB, R_SIBMETA, R_PAIR, R_LAND = 8 * PARTS, 8 * PARTS + 8, 8 * PARTS + 16, 8 * PARTS + 24, 8 * PARTS + 32


def fused_kernel(
    sizes, stream, gain, meta_in, wg_hbm, wu_hbm, wd_hbm, sg_hbm, su_hbm, sd_hbm, out,
    tok0, tok1, mine, meta, pair_in, flow_in, wg, wu, wd, inc, slot_gate, place, shared,
    send_sem, recv_sem, load_sem,
):
    n, local_count, capacity, top = sizes
    rows, width = stream.shape
    part_rows = rows // PARTS
    me = lax.axis_index("ep")
    z, y, core = me // 4, (me // 2) % 2, me % 2
    z_next = z + 1 - 2 * (z % 2)
    is_corner = z * (3 - z) == 0
    peers = {
        "A": z_next * 4 + y * 2 + core,
        "C": z_next * 4 + y * 2 + core,
        "B": z * 4 + (1 - y) * 2 + core,
        "D": z * 4 + (1 - y) * 2 + core,
        "E": (3 - z) * 4 + y * 2 + core,
    }
    sibling = z * 4 + y * 2 + 1 - core

    def when_role(role):
        return pl.when(is_corner if role == "A" else jnp.logical_not(is_corner))

    barrier = pltpu.get_barrier_semaphore()

    def greet(who):
        pl.semaphore_signal(
            barrier, inc=1, device_id={"ep": who}, device_id_type=pl.DeviceIdType.MESH
        )

    greet(sibling)
    greet(peers["A"])
    greet(peers["B"])

    @when_role("C")
    def _():
        greet(peers["E"])

    loads = [
        pltpu.make_async_copy(src, dst, load_sem.at[i])
        for i, (src, dst) in enumerate(
            [
                (sg_hbm, wg.at[1]), (su_hbm, wu.at[1]), (sd_hbm, wd.at[1]),
                (wg_hbm.at[0], wg.at[0]), (wu_hbm.at[0], wu.at[0]), (wd_hbm.at[0], wd.at[0]),
                (wg_hbm.at[1], wg.at[1]), (wu_hbm.at[1], wu.at[1]), (wd_hbm.at[1], wd.at[1]),
            ]
        )
    ]
    for load in loads[:6]:
        load.start()

    def remote(src, dst, send, recv, peer):
        return pltpu.make_async_remote_copy(
            src_ref=src, dst_ref=dst, send_sem=send_sem.at[send], recv_sem=recv_sem.at[recv],
            device_id={"ep": peer}, device_id_type=pl.DeviceIdType.MESH,
        )

    def span_of(part):
        return pl.ds(int(part) * part_rows, part_rows)

    def sibling_copies(slot):
        return (
            remote(meta.at[slot, 0], meta.at[slot, 1], slot, R_SIBMETA + slot, sibling),
            remote(tok0.at[slot], tok1.at[slot], 8 + slot, R_SIB + slot, sibling),
        )

    def pair_copy(slot):
        return remote(tok1.at[slot], pair_in.at[slot], 16 + slot, R_PAIR + slot, sibling)

    piece = 16

    def add_rows(dst, begin, count, others, onto=None):
        def step(i, carry):
            offset = pl.multiple_of(i * piece, piece)
            span = pl.ds(begin + offset, piece)
            total = dst[span, :].astype(jnp.float32)
            for other, start in others:
                total = total + other[pl.ds(start + offset, piece), :].astype(jnp.float32)
            if onto is None:
                dst[span, :] = total.astype(jnp.bfloat16)
            else:
                out[span, :] = (total + onto[span, :]).astype(jnp.bfloat16)
            return carry

        lax.fori_loop(0, count // piece, step, 0)

    class Walk:
        def __init__(self, role):
            self.role, self.own, self.slots = role, role, SLOT[role]
            self.waited, self.used, self.copies = set(), 24, []

        def arrived(self, src, recv, key):
            if key not in self.waited:
                self.waited.add(key)
                remote(src, src, 0, recv, sibling).wait_recv()

        def tokens(self, block, part):
            slot = self.slots[block]
            if block != self.own:
                self.arrived(tok0.at[slot, span_of(part)], slot * PARTS + int(part), ("t", block, part))

        def details(self, block):
            slot = self.slots[block]
            if block != self.own:
                self.arrived(meta.at[slot, 0], R_META + slot, ("m", block))

        def push(self, views, recv, to):
            send, self.used = self.used, self.used + 1

            def copy():
                src, dst = views()
                return remote(src, dst, send, recv, peers[to])

            self.copies.append(copy)
            copy().start()

        def summed(self, block, part, last=False):
            slot, span = self.slots[block], span_of(part)
            others = []
            self.arrived(pair_in.at[slot], R_PAIR + slot, ("p", block))
            others.append((pair_in.at[slot], int(part) * part_rows))
            for (name, which, _, _), k in LANDING[self.role].items():
                if (name, which) == (block, part):
                    self.arrived(flow_in.at[k], R_LAND + k, ("l", k))
                    others.append((flow_in.at[k], 0))
            add_rows(mine.at[slot], int(part) * part_rows, part_rows, others, shared if last else None)

        def run(self, step):
            if step[0] == "g":
                to, block, part = step[1:]
                there, name = seen_from(self.role, to, block)
                slot, target = self.slots[block], SLOT[there][name]
                if part == "0":
                    self.details(block)
                    self.push(lambda: (meta.at[slot, 0], meta.at[target, 0]), R_META + target, to)
                self.tokens(block, part)
                self.push(
                    lambda: (tok0.at[slot, span_of(part)], tok0.at[target, span_of(part)]),
                    target * PARTS + int(part), to,
                )
            elif step[0] == "x":
                block = step[1]
                self.details(block)
                for part in range(PARTS):
                    self.tokens(block, str(part))
                for copy in sibling_copies(self.slots[block]):
                    copy.start()
            elif step[0] == "r":
                to, block, part = step[1:]
                there, name = seen_from(self.role, to, block)
                self.summed(block, part)
                k = LANDING[there][(name, part, self.role, to)]
                slot = self.slots[block]
                self.push(lambda: (mine.at[slot, span_of(part)], flow_in.at[k]), R_LAND + k, to)
            elif step[0] == "f":
                self.summed(step[1], step[2], last=True)

    walks = {role: Walk(role) for role in PLANS}
    segments = {}
    for role, plan in PLANS.items():
        parts = [[]]
        for step in plan:
            if step[0] == "s":
                parts.append([])
            else:
                parts[-1].append(step)
        own_first = [s for s in parts[0] if s[0] in "gx" and s[1 + (s[0] == "g")] == role]
        segments[role] = [own_first, [s for s in parts[0] if s not in own_first]] + parts[1:]

    def run_segment(role, i):
        for step in segments[role][i]:
            walks[role].run(step)

    norm_piece = 32

    def norm_into(slot):
        def norm_rows(i, carry):
            span = pl.ds(pl.multiple_of(i * norm_piece, norm_piece), norm_piece)
            wide = stream[span, :].astype(jnp.float32)
            mean = jnp.mean(wide, axis=-1, keepdims=True)
            centred = wide - mean
            var = jnp.mean(centred * centred, axis=-1, keepdims=True)
            tok0[slot, span, :] = (centred * lax.rsqrt(var + 1e-05) * gain[...]).astype(jnp.bfloat16)
            return carry

        lax.fori_loop(0, rows // norm_piece, norm_rows, 0)
        meta[slot, 0] = meta_in[...]

    own_slot = lax.select(is_corner, SLOT["A"]["A"], SLOT["C"]["C"])
    norm_into(own_slot)

    @when_role("A")
    def _():
        pl.semaphore_wait(barrier, 3)
        run_segment("A", 0)

    @when_role("C")
    def _():
        pl.semaphore_wait(barrier, 4)
        run_segment("C", 0)

    def hidden_of(x, slot):
        gate = jnp.dot(x, wg[slot], preferred_element_type=jnp.float32)
        up = jnp.dot(x, wu[slot], preferred_element_type=jnp.float32)
        return jax.nn.silu(gate) * up

    cols = width // 4

    for load in loads[:3]:
        load.wait()
    hidden = hidden_of(tok0[own_slot], 1).astype(jnp.bfloat16)
    for c in range(4):
        part = pl.ds(c * cols, cols)
        shared[:, part] = jnp.dot(hidden, wd[1, :, part], preferred_element_type=jnp.float32)
    for load in loads[6:]:
        load.start()

    first = (me * local_count).astype(jnp.float32)
    tri = (
        lax.broadcasted_iota(jnp.int32, (rows, rows), 0)
        < lax.broadcasted_iota(jnp.int32, (rows, rows), 1)
    ).astype(jnp.float32).astype(jnp.bfloat16)
    slots = local_count * capacity
    slot_row = lax.broadcasted_iota(jnp.int32, (slots, rows), 0).astype(jnp.float32)
    stack_row = lax.broadcasted_iota(jnp.int32, (8, rows), 0)

    def serve(g):
        stacked = jnp.zeros((8, rows), jnp.float32)
        gate_rows, hit_rows = [], []
        for r in range(2):
            m = meta[g, r]
            ids, weights = m[0:top], m[top:2 * top]
            for x in range(local_count):
                match = (ids == first + x).astype(jnp.float32)
                hit = jnp.sum(match, axis=0, keepdims=True)
                hit_rows.append(hit)
                gate_rows.append(jnp.sum(match * weights, axis=0, keepdims=True))
                stacked = jnp.where(stack_row == r * local_count + x, hit, stacked)
        prior = jnp.dot(stacked.astype(jnp.bfloat16), tri, preferred_element_type=jnp.float32)
        for r in range(2):
            chosen = jnp.zeros((slots, rows), jnp.float32)
            weighted = jnp.zeros((slots, rows), jnp.float32)
            for x in range(local_count):
                q = r * local_count + x
                row = jnp.where(hit_rows[q] > 0, prior[q:q + 1] + x * capacity, -1.0)
                same = (slot_row == row).astype(jnp.float32)
                chosen = chosen + same
                weighted = weighted + same * gate_rows[q]
            slot_gate[r] = jnp.broadcast_to(jnp.sum(weighted, axis=1, keepdims=True), (slots, 128))
            place[r] = chosen.astype(jnp.bfloat16)
            source = tok0 if r == 0 else tok1
            for c in range(4):
                part = pl.ds(c * cols, cols)
                inc[r, :, part] = jnp.dot(
                    place[r], source[g, :, part], preferred_element_type=jnp.float32
                ).astype(jnp.bfloat16)
        for x in range(local_count):
            held = pl.ds(x * capacity, capacity)
            taken = inc[:, held, :].reshape(2 * capacity, width)
            scale = slot_gate[:, held, :].reshape(2 * capacity, 128)[:, 0:1]
            act = (hidden_of(taken, x) * scale).astype(jnp.bfloat16)
            for c in range(4):
                part = pl.ds(c * cols, cols)
                made = jnp.dot(act, wd[x, :, part], preferred_element_type=jnp.float32)
                inc[:, held, part] = made.astype(jnp.bfloat16).reshape(2, capacity, cols)
        for r in (1, 0):
            for c in range(4):
                part = pl.ds(c * cols, cols)
                total = lax.dot_general(
                    place[r], inc[r, :, part], (((0,), (0,)), ((), ())),
                    preferred_element_type=jnp.float32,
                ).astype(jnp.bfloat16)
                if r == 0:
                    mine[g, :, part] = total
                else:
                    tok1[g, :, part] = total
            if r == 1:
                pair_copy(g).start()

    def block(g, carry):
        for i in range(8):
            for role in PLANS:
                @pl.when((g == i) & (is_corner if role == "A" else jnp.logical_not(is_corner)))
                def _():
                    run_segment(role, i + 1)

        @pl.when(g == 0)
        def _():
            for load in loads[3:]:
                load.wait()

        for copy in sibling_copies(g):
            copy.wait_recv()
        serve(g)
        return carry

    lax.fori_loop(0, 8, block, 0)

    for role in PLANS:
        @when_role(role)
        def _():
            run_segment(role, 9)
            for copy in walks[role].copies:
                copy().wait_send()

    def drain(g, carry):
        for copy in sibling_copies(g) + (pair_copy(g),):
            copy.wait_send()
        return carry

    lax.fori_loop(0, 8, drain, 0)


def fused_device(
    stream, norm_gain, routing, gates, w_gate, w_up, w_down, shared_gate, shared_up, shared_down
):
    rows, width = stream.shape
    top = routing.shape[1]
    local_count, _, hidden = w_gate.shape
    n = lax.axis_size("ep")
    capacity = 2 * rows * top // (local_count * n)
    slots = local_count * capacity
    meta = jnp.concatenate([routing.astype(jnp.float32), gates], axis=1).T
    bf16, f32 = jnp.bfloat16, jnp.float32
    vmem, anywhere = pl.BlockSpec(memory_space=pltpu.VMEM), pl.BlockSpec(memory_space=pl.ANY)
    return pl.pallas_call(
        functools.partial(fused_kernel, (n, local_count, capacity, top)),
        out_shape=jax.ShapeDtypeStruct((rows, width), bf16),
        in_specs=[vmem] * 3 + [anywhere] * 6,
        out_specs=vmem,
        scratch_shapes=[
            pltpu.VMEM((8, rows, width), bf16),
            pltpu.VMEM((8, rows, width), bf16),
            pltpu.VMEM((8, rows, width), bf16),
            pltpu.VMEM((8, 2, 2 * top, rows), f32),
            pltpu.VMEM((8, rows, width), bf16),
            pltpu.VMEM((LANDINGS, rows // PARTS, width), bf16),
            pltpu.VMEM((2, width, hidden), bf16),
            pltpu.VMEM((2, width, hidden), bf16),
            pltpu.VMEM((2, hidden, width), bf16),
            pltpu.VMEM((2, slots, width), bf16),
            pltpu.VMEM((2, slots, 128), f32),
            pltpu.VMEM((2, slots, rows), bf16),
            pltpu.VMEM((rows, width), f32),
            pltpu.SemaphoreType.DMA((SENDS,)),
            pltpu.SemaphoreType.DMA((R_LAND + LANDINGS,)),
            pltpu.SemaphoreType.DMA((9,)),
        ],
        compiler_params=pltpu.CompilerParams(
            collective_id=0, has_side_effects=True, vmem_limit_bytes=63 * 1024 * 1024
        ),
    )(stream, norm_gain.reshape(1, -1), meta, w_gate, w_up, w_down, shared_gate, shared_up, shared_down)


def on_device(stream, norm_gain, routing, gates, w_gate, *rest):
    ring = lax.axis_size("ep") // 4
    fits = ring == 4 and w_gate.shape[0] == 2 and rest[2].shape == w_gate.shape[1:]
    run = fused_device if fits else generic_device
    return run(stream, norm_gain, routing, gates, w_gate, *rest)


def solution(mesh):
    placed = (
        P(("grp", "ep"), None),
        P(),
        P(("grp", "ep"), None),
        P(("grp", "ep"), None),
        P("ep", None, None),
        P("ep", None, None),
        P("ep", None, None),
        P(),
        P(),
        P(),
    )
    return jax.shard_map(
        on_device, mesh=mesh, in_specs=placed, out_specs=P(("grp", "ep"), None), check_vma=False
    )
```

```python
import functools
import jax
import jax.numpy as jnp
from jax import lax
from jax.experimental import pallas as pl
from jax.experimental.pallas import tpu as pltpu
from jax.sharding import PartitionSpec as P


def layer_norm(stream, norm_gain):
    widened = stream.astype(jnp.float32)
    row_mean = jnp.mean(widened, axis=-1, keepdims=True)
    variance = jnp.mean(jnp.square(widened - row_mean), axis=-1, keepdims=True)
    return ((widened - row_mean) * lax.rsqrt(variance + 1e-05) * norm_gain).astype(jnp.bfloat16)


def shared_branch(normed, shared_gate, shared_up, shared_down):
    shared_hidden = (
        jax.nn.silu(jnp.dot(normed, shared_gate, preferred_element_type=jnp.float32))
        * jnp.dot(normed, shared_up, preferred_element_type=jnp.float32)
    ).astype(jnp.bfloat16)
    return jnp.dot(shared_hidden, shared_down, preferred_element_type=jnp.float32)


def serve_rows(received, w_gate, w_up, w_down):
    local_count = w_gate.shape[0]
    blocks = received.reshape((-1, local_count) + received.shape[1:])
    gate_act = jnp.einsum("sxcd,xdh->sxch", blocks, w_gate, preferred_element_type=jnp.float32)
    up_act = jnp.einsum("sxcd,xdh->sxch", blocks, w_up, preferred_element_type=jnp.float32)
    hidden = (jax.nn.silu(gate_act) * up_act).astype(jnp.bfloat16)
    produced = jnp.einsum(
        "sxch,xhd->sxcd", hidden, w_down, preferred_element_type=jnp.float32
    ).astype(jnp.bfloat16)
    return lax.all_to_all(
        produced.reshape(received.shape), "ep", split_axis=0, concat_axis=0, tiled=True
    )


def generic_device(
    stream, norm_gain, routing, gates, w_gate, w_up, w_down, shared_gate, shared_up, shared_down
):
    tok_rows, top_count = routing.shape
    local_count = w_gate.shape[0]
    peer_count = lax.axis_size("ep")
    experts = local_count * peer_count
    capacity = 2 * tok_rows * top_count // experts
    normed = layer_norm(stream, norm_gain)
    row_ids = jnp.arange(tok_rows, dtype=jnp.int32)
    lower = (row_ids[:, None] > row_ids[None, :]).astype(jnp.bfloat16)
    slot_ids = jnp.arange(capacity, dtype=jnp.int32).astype(jnp.float32)
    expert_hits = (
        routing[:, :, None] == jnp.arange(experts, dtype=jnp.int32)[None, None, :]
    ).astype(jnp.float32)
    token_hits = jnp.sum(expert_hits, axis=1).astype(jnp.bfloat16)
    earlier = jnp.dot(lower, token_hits, preferred_element_type=jnp.float32)
    slot_index = jnp.sum(earlier[:, None, :] * expert_hits, axis=2)
    slot_hits = (slot_index[:, :, None] == slot_ids[None, None, :]).astype(jnp.float32)
    gate_table = jnp.sum(
        gates[:, :, None, None] * expert_hits[:, :, :, None] * slot_hits[:, :, None, :], axis=1
    )
    all_normed = lax.all_gather(normed, "ep", axis=0, tiled=True)
    all_routing = lax.all_gather(routing, "ep", axis=0, tiled=True)
    first_expert = lax.axis_index("ep") * local_count
    shifted = all_routing.reshape(peer_count, tok_rows, top_count) - first_expert
    local_hits = (
        shifted[:, :, :, None] == jnp.arange(local_count, dtype=jnp.int32)[None, None, None, :]
    ).astype(jnp.float32)
    hits_here = jnp.sum(local_hits, axis=2).astype(jnp.bfloat16)
    prior_here = jnp.einsum("ab,pbx->pax", lower, hits_here, preferred_element_type=jnp.float32)
    placing_here = (
        hits_here.astype(jnp.float32)[:, :, :, None]
        * (prior_here[:, :, :, None] == slot_ids[None, None, None, :]).astype(jnp.float32)
    ).astype(jnp.bfloat16)
    sources = all_normed.reshape(peer_count, tok_rows, all_normed.shape[1])
    incoming = jnp.einsum(
        "ptxc,ptd->pxcd", placing_here, sources, preferred_element_type=jnp.float32
    ).astype(jnp.bfloat16)
    returned = serve_rows(
        incoming.reshape(peer_count * local_count, capacity, all_normed.shape[1]),
        w_gate,
        w_up,
        w_down,
    )
    weight_high = gate_table.astype(jnp.bfloat16)
    weight_low = (gate_table - weight_high.astype(jnp.float32)).astype(jnp.bfloat16)
    routed = jnp.einsum("tec,ecd->td", weight_high, returned, preferred_element_type=jnp.float32)
    routed = routed + jnp.einsum(
        "tec,ecd->td", weight_low, returned, preferred_element_type=jnp.float32
    )
    shared = shared_branch(normed, shared_gate, shared_up, shared_down)
    return (routed + shared).astype(jnp.bfloat16)


CORNER = (
    "gBA0", "gCA1", "gCA2", "gBA1", "gCA3", "xA", "gBC3", "gBA2", "gCB0", "gCB1", "gBC0", "gBC2",
    "gBA3", "gCB2", "xC", "sC", "sA", "rCC1", "gBG1", "gCD2", "xD", "sD", "gBG2", "xB",
    "rCD1", "rBD3", "rBD0", "xH", "sH", "rCC3", "rBH2", "rCH3", "rBH1", "rCH0", "xG", "sG",
    "sB", "gBF3", "rCG0", "gBE0", "rCG1", "rCG3", "rCG2", "rCC0", "gBE1", "rBB3", "xE", "sE",
    "xF", "sF", "rBE3", "rCF2", "rBF1", "rBB2", "rBF0", "rBD2", "rCF3", "rCE1", "rCE2", "fA2",
    "rBB0", "rBB1", "rCE0", "rCC2", "fA0", "fA3", "fA1",
)
MIDDLE = (
    "xC", "gAC3", "gDC3", "gEC3", "gEC1", "gDC0", "gAC2", "gAC0", "gDC1", "gAC1", "sC", "gED3",
    "gEA1", "gDE1", "gEA2", "gAD1", "gDA3", "gDB0", "gAG1", "gEB0", "gAG2", "gEB3", "gEB1", "gDH0",
    "gAH0", "gEB2", "gEC0", "gEC2", "xB", "xA", "sB", "gDH3", "gAH3", "gAG0", "xD", "gAG3",
    "gAF3", "xG", "sG", "sD", "gDE0", "gAE0", "gAE1", "xH", "gDE2", "gAE2", "xE", "sE",
    "sA", "sH", "rEE3", "gAF2", "rAD2", "xF", "sF", "rEH1", "rDA0", "rEH2", "rDF1", "rDG0",
    "rEG1", "rAB1", "rDG3", "rDD1", "rDF0", "rAB2", "rEG2", "rAA1", "rEH0", "rEH3", "rAA2", "rDF2",
    "rAB0", "rEF3", "rDB3", "rEE1", "rDD3", "rDD0", "rEE2", "rAA3", "fC1", "rEE0", "fC3", "fC2",
    "fC0",
)

PLANS = {"A": CORNER, "C": MIDDLE}
PARTS = 4


def across(block):
    return chr(65 + ((ord(block) - 65) ^ 1))


def ahead(block):
    n = ord(block) - 65
    return chr(65 + (3 - n // 2) * 2 + n % 2)


def seen_from(role, to, block):
    if to in ("A", "C"):
        return to, block
    if to in ("B", "D"):
        return role, across(block)
    return role, ahead(block)


SLOT = {role: {s[1]: i for i, s in enumerate([s for s in plan if s[0] == "s"])} for role, plan in PLANS.items()}
LANDING = {"A": {}, "C": {}}
for _role, _plan in PLANS.items():
    for _step in _plan:
        if _step[0] == "r":
            _there, _name = seen_from(_role, _step[1], _step[2])
            LANDING[_there][(_name, _step[3], _role, _step[1])] = len(LANDING[_there])
LANDINGS = max(len(v) for v in LANDING.values())
SENDS = 24 + max(sum(2 if s[0] == "g" else 1 for s in plan) for plan in PLANS.values())
R_META, R_SIB, R_SIBMETA, R_PAIR, R_LAND = 8 * PARTS, 8 * PARTS + 8, 8 * PARTS + 16, 8 * PARTS + 24, 8 * PARTS + 32


def fused_kernel(
    sizes, stream, gain, routing, gates, wg_hbm, wu_hbm, wd_hbm, sg_hbm, su_hbm, sd_hbm, out,
    tok0, tok1, mine, meta, pair_in, flow_in, wg, wu, wd, inc, slot_gate, place, shared,
    send_sem, recv_sem, load_sem,
):
    n, local_count, capacity, top = sizes
    rows, width = stream.shape
    part_rows = rows // PARTS
    me = lax.axis_index("ep")
    z, y, core = me // 4, (me // 2) % 2, me % 2
    z_next = z + 1 - 2 * (z % 2)
    is_corner = z * (3 - z) == 0
    peers = {
        "A": z_next * 4 + y * 2 + core,
        "C": z_next * 4 + y * 2 + core,
        "B": z * 4 + (1 - y) * 2 + core,
        "D": z * 4 + (1 - y) * 2 + core,
        "E": (3 - z) * 4 + y * 2 + core,
    }
    sibling = z * 4 + y * 2 + 1 - core

    def when_role(role):
        return pl.when(is_corner if role == "A" else jnp.logical_not(is_corner))

    barrier = pltpu.get_barrier_semaphore()

    def greet(who):
        pl.semaphore_signal(
            barrier, inc=1, device_id={"ep": who}, device_id_type=pl.DeviceIdType.MESH
        )

    greet(sibling)
    greet(peers["A"])
    greet(peers["B"])

    @when_role("C")
    def _():
        greet(peers["E"])

    loads = [
        pltpu.make_async_copy(src, dst, load_sem.at[i])
        for i, (src, dst) in enumerate(
            [
                (sg_hbm, wg.at[1]), (su_hbm, wu.at[1]), (sd_hbm, wd.at[1]),
                (wg_hbm.at[0], wg.at[0]), (wu_hbm.at[0], wu.at[0]), (wd_hbm.at[0], wd.at[0]),
                (wg_hbm.at[1], wg.at[1]), (wu_hbm.at[1], wu.at[1]), (wd_hbm.at[1], wd.at[1]),
            ]
        )
    ]
    for load in loads[:6]:
        load.start()

    def remote(src, dst, send, recv, peer):
        return pltpu.make_async_remote_copy(
            src_ref=src, dst_ref=dst, send_sem=send_sem.at[send], recv_sem=recv_sem.at[recv],
            device_id={"ep": peer}, device_id_type=pl.DeviceIdType.MESH,
        )

    def span_of(part):
        return pl.ds(int(part) * part_rows, part_rows)

    def sibling_copies(slot):
        return (
            remote(meta.at[slot, 0], meta.at[slot, 1], slot, R_SIBMETA + slot, sibling),
            remote(tok0.at[slot], tok1.at[slot], 8 + slot, R_SIB + slot, sibling),
        )

    def pair_copy(slot):
        return remote(tok1.at[slot], pair_in.at[slot], 16 + slot, R_PAIR + slot, sibling)

    piece = 16

    def add_rows(dst, begin, count, others, onto=None):
        def step(i, carry):
            offset = pl.multiple_of(i * piece, piece)
            span = pl.ds(begin + offset, piece)
            total = dst[span, :].astype(jnp.float32)
            for other, start in others:
                total = total + other[pl.ds(start + offset, piece), :].astype(jnp.float32)
            if onto is None:
                dst[span, :] = total.astype(jnp.bfloat16)
            else:
                out[span, :] = (total + onto[span, :]).astype(jnp.bfloat16)
            return carry

        lax.fori_loop(0, count // piece, step, 0)

    class Walk:
        def __init__(self, role):
            self.role, self.own, self.slots = role, role, SLOT[role]
            self.waited, self.used, self.copies = set(), 24, []

        def arrived(self, src, recv, key):
            if key not in self.waited:
                self.waited.add(key)
                remote(src, src, 0, recv, sibling).wait_recv()

        def tokens(self, block, part):
            slot = self.slots[block]
            if block != self.own:
                self.arrived(tok0.at[slot, span_of(part)], slot * PARTS + int(part), ("t", block, part))

        def details(self, block):
            slot = self.slots[block]
            if block != self.own:
                self.arrived(meta.at[slot, 0], R_META + slot, ("m", block))

        def push(self, views, recv, to):
            send, self.used = self.used, self.used + 1

            def copy():
                src, dst = views()
                return remote(src, dst, send, recv, peers[to])

            self.copies.append(copy)
            copy().start()

        def summed(self, block, part, last=False):
            slot, span = self.slots[block], span_of(part)
            others = []
            self.arrived(pair_in.at[slot], R_PAIR + slot, ("p", block))
            others.append((pair_in.at[slot], int(part) * part_rows))
            for (name, which, _, _), k in LANDING[self.role].items():
                if (name, which) == (block, part):
                    self.arrived(flow_in.at[k], R_LAND + k, ("l", k))
                    others.append((flow_in.at[k], 0))
            add_rows(mine.at[slot], int(part) * part_rows, part_rows, others, shared if last else None)

        def run(self, step):
            if step[0] == "g":
                to, block, part = step[1:]
                there, name = seen_from(self.role, to, block)
                slot, target = self.slots[block], SLOT[there][name]
                if part == "0":
                    self.details(block)
                    self.push(lambda: (meta.at[slot, 0], meta.at[target, 0]), R_META + target, to)
                self.tokens(block, part)
                self.push(
                    lambda: (tok0.at[slot, span_of(part)], tok0.at[target, span_of(part)]),
                    target * PARTS + int(part), to,
                )
            elif step[0] == "x":
                block = step[1]
                self.details(block)
                for part in range(PARTS):
                    self.tokens(block, str(part))
                for copy in sibling_copies(self.slots[block]):
                    copy.start()
            elif step[0] == "r":
                to, block, part = step[1:]
                there, name = seen_from(self.role, to, block)
                self.summed(block, part)
                k = LANDING[there][(name, part, self.role, to)]
                slot = self.slots[block]
                self.push(lambda: (mine.at[slot, span_of(part)], flow_in.at[k]), R_LAND + k, to)
            elif step[0] == "f":
                self.summed(step[1], step[2], last=True)

    walks = {role: Walk(role) for role in PLANS}
    segments = {}
    for role, plan in PLANS.items():
        parts = [[]]
        for step in plan:
            if step[0] == "s":
                parts.append([])
            else:
                parts[-1].append(step)
        own_first = [s for s in parts[0] if s[0] in "gx" and s[1 + (s[0] == "g")] == role]
        segments[role] = [own_first, [s for s in parts[0] if s not in own_first]] + parts[1:]

    def run_segment(role, i):
        for step in segments[role][i]:
            walks[role].run(step)

    norm_piece = 32

    def norm_into(slot):
        def norm_rows(i, carry):
            span = pl.ds(pl.multiple_of(i * norm_piece, norm_piece), norm_piece)
            wide = stream[span, :].astype(jnp.float32)
            mean = jnp.mean(wide, axis=-1, keepdims=True)
            centred = wide - mean
            var = jnp.mean(centred * centred, axis=-1, keepdims=True)
            tok0[slot, span, :] = (centred * lax.rsqrt(var + 1e-05) * gain[...]).astype(jnp.bfloat16)
            return carry

        lax.fori_loop(0, rows // norm_piece, norm_rows, 0)
        meta[slot, 0, 0:top] = routing[...].astype(jnp.float32)
        meta[slot, 0, top:2 * top] = gates[...]

    own_slot = lax.select(is_corner, SLOT["A"]["A"], SLOT["C"]["C"])
    norm_into(own_slot)

    @when_role("A")
    def _():
        pl.semaphore_wait(barrier, 3)
        run_segment("A", 0)

    @when_role("C")
    def _():
        pl.semaphore_wait(barrier, 4)
        run_segment("C", 0)

    def hidden_of(x, slot):
        gate = jnp.dot(x, wg[slot], preferred_element_type=jnp.float32)
        up = jnp.dot(x, wu[slot], preferred_element_type=jnp.float32)
        return jax.nn.silu(gate) * up

    cols = width // 4

    for load in loads[:3]:
        load.wait()
    hidden = hidden_of(tok0[own_slot], 1).astype(jnp.bfloat16)
    for c in range(4):
        part = pl.ds(c * cols, cols)
        shared[:, part] = jnp.dot(hidden, wd[1, :, part], preferred_element_type=jnp.float32)
    for load in loads[6:]:
        load.start()

    first = (me * local_count).astype(jnp.float32)
    tri = (
        lax.broadcasted_iota(jnp.int32, (rows, rows), 0)
        < lax.broadcasted_iota(jnp.int32, (rows, rows), 1)
    ).astype(jnp.float32).astype(jnp.bfloat16)
    slots = local_count * capacity
    slot_row = lax.broadcasted_iota(jnp.int32, (slots, rows), 0).astype(jnp.float32)
    stack_row = lax.broadcasted_iota(jnp.int32, (8, rows), 0)

    def serve(g):
        stacked = jnp.zeros((8, rows), jnp.float32)
        gate_rows, hit_rows = [], []
        for r in range(2):
            m = meta[g, r]
            ids, weights = m[0:top], m[top:2 * top]
            for x in range(local_count):
                match = (ids == first + x).astype(jnp.float32)
                hit = jnp.sum(match, axis=0, keepdims=True)
                hit_rows.append(hit)
                gate_rows.append(jnp.sum(match * weights, axis=0, keepdims=True))
                stacked = jnp.where(stack_row == r * local_count + x, hit, stacked)
        prior = jnp.dot(stacked.astype(jnp.bfloat16), tri, preferred_element_type=jnp.float32)
        for r in range(2):
            chosen = jnp.zeros((slots, rows), jnp.float32)
            weighted = jnp.zeros((slots, rows), jnp.float32)
            for x in range(local_count):
                q = r * local_count + x
                row = jnp.where(hit_rows[q] > 0, prior[q:q + 1] + x * capacity, -1.0)
                same = (slot_row == row).astype(jnp.float32)
                chosen = chosen + same
                weighted = weighted + same * gate_rows[q]
            slot_gate[r] = jnp.broadcast_to(jnp.sum(weighted, axis=1, keepdims=True), (slots, 128))
            place[r] = chosen.astype(jnp.bfloat16)
            source = tok0 if r == 0 else tok1
            for c in range(4):
                part = pl.ds(c * cols, cols)
                inc[r, :, part] = jnp.dot(
                    place[r], source[g, :, part], preferred_element_type=jnp.float32
                ).astype(jnp.bfloat16)
        for x in range(local_count):
            held = pl.ds(x * capacity, capacity)
            taken = inc[:, held, :].reshape(2 * capacity, width)
            scale = slot_gate[:, held, :].reshape(2 * capacity, 128)[:, 0:1]
            act = (hidden_of(taken, x) * scale).astype(jnp.bfloat16)
            for c in range(4):
                part = pl.ds(c * cols, cols)
                made = jnp.dot(act, wd[x, :, part], preferred_element_type=jnp.float32)
                inc[:, held, part] = made.astype(jnp.bfloat16).reshape(2, capacity, cols)
        for r in (1, 0):
            for c in range(4):
                part = pl.ds(c * cols, cols)
                total = lax.dot_general(
                    place[r], inc[r, :, part], (((0,), (0,)), ((), ())),
                    preferred_element_type=jnp.float32,
                ).astype(jnp.bfloat16)
                if r == 0:
                    mine[g, :, part] = total
                else:
                    tok1[g, :, part] = total
            if r == 1:
                pair_copy(g).start()

    def block(g, carry):
        for i in range(8):
            for role in PLANS:
                @pl.when((g == i) & (is_corner if role == "A" else jnp.logical_not(is_corner)))
                def _():
                    run_segment(role, i + 1)

        @pl.when(g == 0)
        def _():
            for load in loads[3:]:
                load.wait()

        for copy in sibling_copies(g):
            copy.wait_recv()
        serve(g)
        return carry

    lax.fori_loop(0, 8, block, 0)

    for role in PLANS:
        @when_role(role)
        def _():
            run_segment(role, 9)
            for copy in walks[role].copies:
                copy().wait_send()

    def drain(g, carry):
        for copy in sibling_copies(g) + (pair_copy(g),):
            copy.wait_send()
        return carry

    lax.fori_loop(0, 8, drain, 0)


def fused_device(
    stream, norm_gain, routing, gates, w_gate, w_up, w_down, shared_gate, shared_up, shared_down
):
    rows, width = stream.shape
    top = routing.shape[1]
    local_count, _, hidden = w_gate.shape
    n = lax.axis_size("ep")
    capacity = 2 * rows * top // (local_count * n)
    slots = local_count * capacity
    bf16, f32 = jnp.bfloat16, jnp.float32
    vmem, anywhere = pl.BlockSpec(memory_space=pltpu.VMEM), pl.BlockSpec(memory_space=pl.ANY)
    return pl.pallas_call(
        functools.partial(fused_kernel, (n, local_count, capacity, top)),
        out_shape=pltpu.VMEM((rows, width), bf16),
        in_specs=[vmem] * 4 + [anywhere] * 6,
        out_specs=vmem,
        scratch_shapes=[
            pltpu.VMEM((8, rows, width), bf16),
            pltpu.VMEM((8, rows, width), bf16),
            pltpu.VMEM((8, rows, width), bf16),
            pltpu.VMEM((8, 2, 2 * top, rows), f32),
            pltpu.VMEM((8, rows, width), bf16),
            pltpu.VMEM((LANDINGS, rows // PARTS, width), bf16),
            pltpu.VMEM((2, width, hidden), bf16),
            pltpu.VMEM((2, width, hidden), bf16),
            pltpu.VMEM((2, hidden, width), bf16),
            pltpu.VMEM((2, slots, width), bf16),
            pltpu.VMEM((2, slots, 128), f32),
            pltpu.VMEM((2, slots, rows), bf16),
            pltpu.VMEM((rows, width), f32),
            pltpu.SemaphoreType.DMA((SENDS,)),
            pltpu.SemaphoreType.DMA((R_LAND + LANDINGS,)),
            pltpu.SemaphoreType.DMA((9,)),
        ],
        compiler_params=pltpu.CompilerParams(
            collective_id=0, has_side_effects=True, vmem_limit_bytes=61 * 1024 * 1024
        ),
    )(
        stream, norm_gain.reshape(1, -1), routing.T, gates.T,
        w_gate, w_up, w_down, shared_gate, shared_up, shared_down,
    )


def on_device(stream, norm_gain, routing, gates, w_gate, *rest):
    ring = lax.axis_size("ep") // 4
    fits = ring == 4 and w_gate.shape[0] == 2 and rest[2].shape == w_gate.shape[1:]
    run = fused_device if fits else generic_device
    return run(stream, norm_gain, routing, gates, w_gate, *rest)


def solution(mesh):
    placed = (
        P(("grp", "ep"), None),
        P(),
        P(("grp", "ep"), None),
        P(("grp", "ep"), None),
        P("ep", None, None),
        P("ep", None, None),
        P("ep", None, None),
        P(),
        P(),
        P(),
    )
    return jax.shard_map(
        on_device, mesh=mesh, in_specs=placed, out_specs=P(("grp", "ep"), None), check_vma=False
    )
```

```python
import functools
import jax
import jax.numpy as jnp
from jax import lax
from jax.experimental import pallas as pl
from jax.experimental.pallas import tpu as pltpu
from jax.sharding import PartitionSpec as P


def layer_norm(stream, norm_gain):
    widened = stream.astype(jnp.float32)
    row_mean = jnp.mean(widened, axis=-1, keepdims=True)
    variance = jnp.mean(jnp.square(widened - row_mean), axis=-1, keepdims=True)
    return ((widened - row_mean) * lax.rsqrt(variance + 1e-05) * norm_gain).astype(jnp.bfloat16)


def shared_branch(normed, shared_gate, shared_up, shared_down):
    shared_hidden = (
        jax.nn.silu(jnp.dot(normed, shared_gate, preferred_element_type=jnp.float32))
        * jnp.dot(normed, shared_up, preferred_element_type=jnp.float32)
    ).astype(jnp.bfloat16)
    return jnp.dot(shared_hidden, shared_down, preferred_element_type=jnp.float32)


def serve_rows(received, w_gate, w_up, w_down):
    local_count = w_gate.shape[0]
    blocks = received.reshape((-1, local_count) + received.shape[1:])
    gate_act = jnp.einsum("sxcd,xdh->sxch", blocks, w_gate, preferred_element_type=jnp.float32)
    up_act = jnp.einsum("sxcd,xdh->sxch", blocks, w_up, preferred_element_type=jnp.float32)
    hidden = (jax.nn.silu(gate_act) * up_act).astype(jnp.bfloat16)
    produced = jnp.einsum(
        "sxch,xhd->sxcd", hidden, w_down, preferred_element_type=jnp.float32
    ).astype(jnp.bfloat16)
    return lax.all_to_all(
        produced.reshape(received.shape), "ep", split_axis=0, concat_axis=0, tiled=True
    )


def generic_device(
    stream, norm_gain, routing, gates, w_gate, w_up, w_down, shared_gate, shared_up, shared_down
):
    tok_rows, top_count = routing.shape
    local_count = w_gate.shape[0]
    peer_count = lax.axis_size("ep")
    experts = local_count * peer_count
    capacity = 2 * tok_rows * top_count // experts
    normed = layer_norm(stream, norm_gain)
    row_ids = jnp.arange(tok_rows, dtype=jnp.int32)
    lower = (row_ids[:, None] > row_ids[None, :]).astype(jnp.bfloat16)
    slot_ids = jnp.arange(capacity, dtype=jnp.int32).astype(jnp.float32)
    expert_hits = (
        routing[:, :, None] == jnp.arange(experts, dtype=jnp.int32)[None, None, :]
    ).astype(jnp.float32)
    token_hits = jnp.sum(expert_hits, axis=1).astype(jnp.bfloat16)
    earlier = jnp.dot(lower, token_hits, preferred_element_type=jnp.float32)
    slot_index = jnp.sum(earlier[:, None, :] * expert_hits, axis=2)
    slot_hits = (slot_index[:, :, None] == slot_ids[None, None, :]).astype(jnp.float32)
    gate_table = jnp.sum(
        gates[:, :, None, None] * expert_hits[:, :, :, None] * slot_hits[:, :, None, :], axis=1
    )
    all_normed = lax.all_gather(normed, "ep", axis=0, tiled=True)
    all_routing = lax.all_gather(routing, "ep", axis=0, tiled=True)
    first_expert = lax.axis_index("ep") * local_count
    shifted = all_routing.reshape(peer_count, tok_rows, top_count) - first_expert
    local_hits = (
        shifted[:, :, :, None] == jnp.arange(local_count, dtype=jnp.int32)[None, None, None, :]
    ).astype(jnp.float32)
    hits_here = jnp.sum(local_hits, axis=2).astype(jnp.bfloat16)
    prior_here = jnp.einsum("ab,pbx->pax", lower, hits_here, preferred_element_type=jnp.float32)
    placing_here = (
        hits_here.astype(jnp.float32)[:, :, :, None]
        * (prior_here[:, :, :, None] == slot_ids[None, None, None, :]).astype(jnp.float32)
    ).astype(jnp.bfloat16)
    sources = all_normed.reshape(peer_count, tok_rows, all_normed.shape[1])
    incoming = jnp.einsum(
        "ptxc,ptd->pxcd", placing_here, sources, preferred_element_type=jnp.float32
    ).astype(jnp.bfloat16)
    returned = serve_rows(
        incoming.reshape(peer_count * local_count, capacity, all_normed.shape[1]),
        w_gate,
        w_up,
        w_down,
    )
    weight_high = gate_table.astype(jnp.bfloat16)
    weight_low = (gate_table - weight_high.astype(jnp.float32)).astype(jnp.bfloat16)
    routed = jnp.einsum("tec,ecd->td", weight_high, returned, preferred_element_type=jnp.float32)
    routed = routed + jnp.einsum(
        "tec,ecd->td", weight_low, returned, preferred_element_type=jnp.float32
    )
    shared = shared_branch(normed, shared_gate, shared_up, shared_down)
    return (routed + shared).astype(jnp.bfloat16)


CORNER = (
    1104, 1102, 1201, 2000, 1103, 1203, 1204, 1105, 1207, 1125, 1126, 1206, 1215, 1200, 1123, 1202,
    1120, 1121, 1212, 1205, 1122, 1106, 1101, 2020, 3020, 2030, 1161, 1216, 1230, 1163, 3030, 1162,
    4227, 1160, 4237, 4234, 4133, 4224, 4132, 3000, 4136, 4131, 4223, 1107, 2070, 1100, 4222, 4226,
    3070, 4221, 4135, 4277, 4170, 4171, 2060, 4172, 4275, 4276, 1143, 3060, 2010, 4274, 1147, 4260,
    1146, 4262, 4261, 3010, 4173, 1155, 1154, 4264, 4266, 2050, 4113, 4265, 4263, 4114, 4267, 3050,
    2040, 4252, 4110, 4251, 4153, 4157, 3040, 4250, 4145, 4156, 4241, 4144, 4243, 4242, 4255, 4111,
    4116, 4254, 4246, 4115, 4247, 4117, 4130, 4112, 4240, 5004, 4225, 5003, 5001, 5000, 5006, 4220,
    5007, 5005, 5002,
)
MIDDLE = (
    1023, 1025, 1321, 1424, 1323, 1427, 1425, 1324, 1026, 1021, 1020, 1420, 1326, 1401, 1327, 1403,
    1404, 1027, 1407, 1022, 1024, 1303, 2020, 1406, 1340, 1361, 1037, 1034, 1325, 1402, 1322, 1061,
    1400, 1367, 1364, 1063, 1422, 1415, 1405, 1300, 1362, 1062, 1366, 1421, 3020, 1307, 1423, 1363,
    1060, 1435, 2000, 1074, 1077, 1426, 2030, 1410, 2060, 1075, 1076, 1065, 1431, 1067, 1347, 1064,
    1434, 1066, 1433, 1301, 1043, 1304, 1342, 3030, 3060, 1046, 2070, 1047, 2040, 3000, 4337, 3040,
    1346, 3070, 1050, 1054, 4373, 1055, 4371, 4372, 1052, 4470, 4445, 4444, 2050, 4336, 1051, 1041,
    4377, 2010, 4475, 1040, 3050, 1042, 4460, 3010, 4030, 4374, 4453, 4462, 4314, 4376, 4464, 4461,
    4015, 4317, 4313, 4466, 4310, 4311, 4004, 4463, 4332, 4002, 4467, 4012, 4451, 4352, 4357, 4016,
    4006, 4003, 4465, 4441, 4001, 4333, 4443, 4000, 4442, 4007, 4356, 4455, 4331, 4350, 4454, 4446,
    4335, 4005, 5021, 4447, 4334, 5022, 4440, 5023, 5024, 5025, 5027, 5026, 5020,
)
PARTS = 8


def step_of(code):
    kind, to, block, part = "gxsrf"[code // 1000 - 1], "ABCDE"[code // 100 % 10], chr(65 + code // 10 % 10), str(code % 10)
    return kind + (to if kind in "gr" else "") + block + (part if kind in "grf" else "")


PLANS = {"A": [step_of(code) for code in CORNER], "C": [step_of(code) for code in MIDDLE]}


def across(block):
    return chr(65 + ((ord(block) - 65) ^ 1))


def ahead(block):
    n = ord(block) - 65
    return chr(65 + (3 - n // 2) * 2 + n % 2)


def seen_from(role, to, block):
    if to in ("A", "C"):
        return to, block
    if to in ("B", "D"):
        return role, across(block)
    return role, ahead(block)


SLOT = {role: {s[1]: i for i, s in enumerate([s for s in plan if s[0] == "s"])} for role, plan in PLANS.items()}
LANDING = {"A": {}, "C": {}}
for _role, _plan in PLANS.items():
    for _step in _plan:
        if _step[0] == "r":
            _there, _name = seen_from(_role, _step[1], _step[2])
            LANDING[_there][(_name, _step[3], _role, _step[1])] = len(LANDING[_there])
LANDINGS = max(len(v) for v in LANDING.values())
SENDS = 24 + max(sum(2 if s[0] == "g" else 1 for s in plan) for plan in PLANS.values())
R_META, R_SIB, R_SIBMETA, R_PAIR, R_LAND = 8 * PARTS, 8 * PARTS + 8, 8 * PARTS + 16, 8 * PARTS + 24, 8 * PARTS + 32


def fused_kernel(
    sizes, stream, gain, routing, gates, wg_hbm, wu_hbm, wd_hbm, sg_hbm, su_hbm, sd_hbm, out,
    tok0, tok1, mine, meta, pair_in, flow_in, wg, wu, wd, inc, slot_gate, place, shared,
    send_sem, recv_sem, load_sem,
):
    n, local_count, capacity, top = sizes
    rows, width = stream.shape
    part_rows = rows // PARTS
    me = lax.axis_index("ep")
    z, y, core = me // 4, (me // 2) % 2, me % 2
    z_next = z + 1 - 2 * (z % 2)
    is_corner = z * (3 - z) == 0
    peers = {
        "A": z_next * 4 + y * 2 + core,
        "C": z_next * 4 + y * 2 + core,
        "B": z * 4 + (1 - y) * 2 + core,
        "D": z * 4 + (1 - y) * 2 + core,
        "E": (3 - z) * 4 + y * 2 + core,
    }
    sibling = z * 4 + y * 2 + 1 - core

    def when_role(role):
        return pl.when(is_corner if role == "A" else jnp.logical_not(is_corner))

    barrier = pltpu.get_barrier_semaphore()

    def greet(who):
        pl.semaphore_signal(
            barrier, inc=1, device_id={"ep": who}, device_id_type=pl.DeviceIdType.MESH
        )

    greet(sibling)
    greet(peers["A"])
    greet(peers["B"])

    @when_role("C")
    def _():
        greet(peers["E"])

    loads = [
        pltpu.make_async_copy(src, dst, load_sem.at[i])
        for i, (src, dst) in enumerate(
            [
                (sg_hbm, wg.at[1]), (su_hbm, wu.at[1]), (sd_hbm, wd.at[1]),
                (wg_hbm.at[0], wg.at[0]), (wu_hbm.at[0], wu.at[0]), (wd_hbm.at[0], wd.at[0]),
                (wg_hbm.at[1], wg.at[1]), (wu_hbm.at[1], wu.at[1]), (wd_hbm.at[1], wd.at[1]),
            ]
        )
    ]
    for load in loads[:6]:
        load.start()

    def remote(src, dst, send, recv, peer):
        return pltpu.make_async_remote_copy(
            src_ref=src, dst_ref=dst, send_sem=send_sem.at[send], recv_sem=recv_sem.at[recv],
            device_id={"ep": peer}, device_id_type=pl.DeviceIdType.MESH,
        )

    def span_of(part):
        return pl.ds(int(part) * part_rows, part_rows)

    def sibling_copies(slot):
        return (
            remote(meta.at[slot, 0], meta.at[slot, 1], slot, R_SIBMETA + slot, sibling),
            remote(tok0.at[slot], tok1.at[slot], 8 + slot, R_SIB + slot, sibling),
        )

    def pair_copy(slot):
        return remote(tok1.at[slot], pair_in.at[slot], 16 + slot, R_PAIR + slot, sibling)

    piece = 16

    def add_rows(dst, begin, count, others, onto=None):
        def step(i, carry):
            offset = pl.multiple_of(i * piece, piece)
            span = pl.ds(begin + offset, piece)
            total = dst[span, :].astype(jnp.float32)
            for other, start in others:
                total = total + other[pl.ds(start + offset, piece), :].astype(jnp.float32)
            if onto is None:
                dst[span, :] = total.astype(jnp.bfloat16)
            else:
                out[span, :] = (total + onto[span, :]).astype(jnp.bfloat16)
            return carry

        lax.fori_loop(0, count // piece, step, 0)

    class Walk:
        def __init__(self, role):
            self.role, self.own, self.slots = role, role, SLOT[role]
            self.waited, self.used, self.copies = set(), 24, []

        def arrived(self, src, recv, key):
            if key not in self.waited:
                self.waited.add(key)
                remote(src, src, 0, recv, sibling).wait_recv()

        def tokens(self, block, part):
            slot = self.slots[block]
            if block != self.own:
                self.arrived(tok0.at[slot, span_of(part)], slot * PARTS + int(part), ("t", block, part))

        def details(self, block):
            slot = self.slots[block]
            if block != self.own:
                self.arrived(meta.at[slot, 0], R_META + slot, ("m", block))

        def push(self, views, recv, to):
            send, self.used = self.used, self.used + 1

            def copy():
                src, dst = views()
                return remote(src, dst, send, recv, peers[to])

            self.copies.append(copy)
            copy().start()

        def summed(self, block, part, last=False):
            slot, span = self.slots[block], span_of(part)
            others = []
            self.arrived(pair_in.at[slot], R_PAIR + slot, ("p", block))
            others.append((pair_in.at[slot], int(part) * part_rows))
            for (name, which, _, _), k in LANDING[self.role].items():
                if (name, which) == (block, part):
                    self.arrived(flow_in.at[k], R_LAND + k, ("l", k))
                    others.append((flow_in.at[k], 0))
            add_rows(mine.at[slot], int(part) * part_rows, part_rows, others, shared if last else None)

        def run(self, step):
            if step[0] == "g":
                to, block, part = step[1:]
                there, name = seen_from(self.role, to, block)
                slot, target = self.slots[block], SLOT[there][name]
                if part == "0":
                    self.details(block)
                    self.push(lambda: (meta.at[slot, 0], meta.at[target, 0]), R_META + target, to)
                self.tokens(block, part)
                self.push(
                    lambda: (tok0.at[slot, span_of(part)], tok0.at[target, span_of(part)]),
                    target * PARTS + int(part), to,
                )
            elif step[0] == "x":
                block = step[1]
                self.details(block)
                for part in range(PARTS):
                    self.tokens(block, str(part))
                for copy in sibling_copies(self.slots[block]):
                    copy.start()
            elif step[0] == "r":
                to, block, part = step[1:]
                there, name = seen_from(self.role, to, block)
                self.summed(block, part)
                k = LANDING[there][(name, part, self.role, to)]
                slot = self.slots[block]
                self.push(lambda: (mine.at[slot, span_of(part)], flow_in.at[k]), R_LAND + k, to)
            elif step[0] == "f":
                self.summed(step[1], step[2], last=True)

    walks = {role: Walk(role) for role in PLANS}
    segments = {}
    for role, plan in PLANS.items():
        parts = [[]]
        for step in plan:
            if step[0] == "s":
                parts.append([])
            else:
                parts[-1].append(step)
        mark = 0
        while mark < len(parts[0]) and parts[0][mark].rstrip("01234567")[-1] == role and parts[0][mark][0] in "gx":
            mark += 1
        segments[role] = [parts[0][:mark], parts[0][mark:]] + parts[1:]

    def run_segment(role, i):
        for step in segments[role][i]:
            walks[role].run(step)

    norm_piece = 32

    def norm_into(slot):
        def norm_rows(i, carry):
            span = pl.ds(pl.multiple_of(i * norm_piece, norm_piece), norm_piece)
            wide = stream[span, :].astype(jnp.float32)
            mean = jnp.mean(wide, axis=-1, keepdims=True)
            centred = wide - mean
            var = jnp.mean(centred * centred, axis=-1, keepdims=True)
            tok0[slot, span, :] = (centred * lax.rsqrt(var + 1e-05) * gain[...]).astype(jnp.bfloat16)
            return carry

        lax.fori_loop(0, rows // norm_piece, norm_rows, 0)
        meta[slot, 0, 0:top] = routing[...].astype(jnp.float32)
        meta[slot, 0, top:2 * top] = gates[...]

    own_slot = lax.select(is_corner, SLOT["A"]["A"], SLOT["C"]["C"])
    norm_into(own_slot)

    @when_role("A")
    def _():
        pl.semaphore_wait(barrier, 3)
        run_segment("A", 0)

    @when_role("C")
    def _():
        pl.semaphore_wait(barrier, 4)
        run_segment("C", 0)

    def hidden_of(x, slot):
        gate = jnp.dot(x, wg[slot], preferred_element_type=jnp.float32)
        up = jnp.dot(x, wu[slot], preferred_element_type=jnp.float32)
        return jax.nn.silu(gate) * up

    cols = width // 4

    for load in loads[:3]:
        load.wait()
    hidden = hidden_of(tok0[own_slot], 1).astype(jnp.bfloat16)
    for c in range(4):
        part = pl.ds(c * cols, cols)
        shared[:, part] = jnp.dot(hidden, wd[1, :, part], preferred_element_type=jnp.float32)
    for load in loads[6:]:
        load.start()

    first = (me * local_count).astype(jnp.float32)
    tri = (
        lax.broadcasted_iota(jnp.int32, (rows, rows), 0)
        < lax.broadcasted_iota(jnp.int32, (rows, rows), 1)
    ).astype(jnp.float32).astype(jnp.bfloat16)
    slots = local_count * capacity
    slot_row = lax.broadcasted_iota(jnp.int32, (slots, rows), 0).astype(jnp.float32)
    stack_row = lax.broadcasted_iota(jnp.int32, (8, rows), 0)

    def serve(g):
        stacked = jnp.zeros((8, rows), jnp.float32)
        gate_rows, hit_rows = [], []
        for r in range(2):
            m = meta[g, r]
            ids, weights = m[0:top], m[top:2 * top]
            for x in range(local_count):
                match = (ids == first + x).astype(jnp.float32)
                hit = jnp.sum(match, axis=0, keepdims=True)
                hit_rows.append(hit)
                gate_rows.append(jnp.sum(match * weights, axis=0, keepdims=True))
                stacked = jnp.where(stack_row == r * local_count + x, hit, stacked)
        prior = jnp.dot(stacked.astype(jnp.bfloat16), tri, preferred_element_type=jnp.float32)
        for r in range(2):
            chosen = jnp.zeros((slots, rows), jnp.float32)
            weighted = jnp.zeros((slots, rows), jnp.float32)
            for x in range(local_count):
                q = r * local_count + x
                row = jnp.where(hit_rows[q] > 0, prior[q:q + 1] + x * capacity, -1.0)
                same = (slot_row == row).astype(jnp.float32)
                chosen = chosen + same
                weighted = weighted + same * gate_rows[q]
            slot_gate[r] = jnp.broadcast_to(jnp.sum(weighted, axis=1, keepdims=True), (slots, 128))
            place[r] = chosen.astype(jnp.bfloat16)
            source = tok0 if r == 0 else tok1
            for c in range(4):
                part = pl.ds(c * cols, cols)
                inc[r, :, part] = jnp.dot(
                    place[r], source[g, :, part], preferred_element_type=jnp.float32
                ).astype(jnp.bfloat16)
        for x in range(local_count):
            held = pl.ds(x * capacity, capacity)
            taken = inc[:, held, :].reshape(2 * capacity, width)
            scale = slot_gate[:, held, :].reshape(2 * capacity, 128)[:, 0:1]
            act = (hidden_of(taken, x) * scale).astype(jnp.bfloat16)
            for c in range(4):
                part = pl.ds(c * cols, cols)
                made = jnp.dot(act, wd[x, :, part], preferred_element_type=jnp.float32)
                inc[:, held, part] = made.astype(jnp.bfloat16).reshape(2, capacity, cols)
        for r in (1, 0):
            for c in range(4):
                part = pl.ds(c * cols, cols)
                total = lax.dot_general(
                    place[r], inc[r, :, part], (((0,), (0,)), ((), ())),
                    preferred_element_type=jnp.float32,
                ).astype(jnp.bfloat16)
                if r == 0:
                    mine[g, :, part] = total
                else:
                    tok1[g, :, part] = total
            if r == 1:
                pair_copy(g).start()

    def block(g, carry):
        for i in range(8):
            for role in PLANS:
                @pl.when((g == i) & (is_corner if role == "A" else jnp.logical_not(is_corner)))
                def _():
                    run_segment(role, i + 1)

        @pl.when(g == 0)
        def _():
            for load in loads[3:]:
                load.wait()

        for copy in sibling_copies(g):
            copy.wait_recv()
        serve(g)
        return carry

    lax.fori_loop(0, 8, block, 0)

    for role in PLANS:
        @when_role(role)
        def _():
            run_segment(role, 9)
            for copy in walks[role].copies:
                copy().wait_send()

    def drain(g, carry):
        for copy in sibling_copies(g) + (pair_copy(g),):
            copy.wait_send()
        return carry

    lax.fori_loop(0, 8, drain, 0)


def fused_device(
    stream, norm_gain, routing, gates, w_gate, w_up, w_down, shared_gate, shared_up, shared_down
):
    rows, width = stream.shape
    top = routing.shape[1]
    local_count, _, hidden = w_gate.shape
    n = lax.axis_size("ep")
    capacity = 2 * rows * top // (local_count * n)
    slots = local_count * capacity
    bf16, f32 = jnp.bfloat16, jnp.float32
    vmem, anywhere = pl.BlockSpec(memory_space=pltpu.VMEM), pl.BlockSpec(memory_space=pl.ANY)
    return pl.pallas_call(
        functools.partial(fused_kernel, (n, local_count, capacity, top)),
        out_shape=pltpu.VMEM((rows, width), bf16),
        in_specs=[vmem] * 4 + [anywhere] * 6,
        out_specs=vmem,
        scratch_shapes=[
            pltpu.VMEM((8, rows, width), bf16),
            pltpu.VMEM((8, rows, width), bf16),
            pltpu.VMEM((8, rows, width), bf16),
            pltpu.VMEM((8, 2, 2 * top, rows), f32),
            pltpu.VMEM((8, rows, width), bf16),
            pltpu.VMEM((LANDINGS, rows // PARTS, width), bf16),
            pltpu.VMEM((2, width, hidden), bf16),
            pltpu.VMEM((2, width, hidden), bf16),
            pltpu.VMEM((2, hidden, width), bf16),
            pltpu.VMEM((2, slots, width), bf16),
            pltpu.VMEM((2, slots, 128), f32),
            pltpu.VMEM((2, slots, rows), bf16),
            pltpu.VMEM((rows, width), f32),
            pltpu.SemaphoreType.DMA((SENDS,)),
            pltpu.SemaphoreType.DMA((R_LAND + LANDINGS,)),
            pltpu.SemaphoreType.DMA((9,)),
        ],
        compiler_params=pltpu.CompilerParams(
            collective_id=0, has_side_effects=True, vmem_limit_bytes=61 * 1024 * 1024
        ),
    )(
        stream, norm_gain.reshape(1, -1), routing.T, gates.T,
        w_gate, w_up, w_down, shared_gate, shared_up, shared_down,
    )


def on_device(stream, norm_gain, routing, gates, w_gate, *rest):
    ring = lax.axis_size("ep") // 4
    fits = ring == 4 and w_gate.shape[0] == 2 and rest[2].shape == w_gate.shape[1:]
    run = fused_device if fits else generic_device
    return run(stream, norm_gain, routing, gates, w_gate, *rest)


def solution(mesh):
    placed = (
        P(("grp", "ep"), None),
        P(),
        P(("grp", "ep"), None),
        P(("grp", "ep"), None),
        P("ep", None, None),
        P("ep", None, None),
        P("ep", None, None),
        P(),
        P(),
        P(),
    )
    return jax.shard_map(
        on_device, mesh=mesh, in_specs=placed, out_specs=P(("grp", "ep"), None), check_vma=False
    )
```

```python
import functools
import jax
import jax.numpy as jnp
from jax import lax
from jax.experimental import pallas as pl
from jax.experimental.pallas import tpu as pltpu
from jax.sharding import PartitionSpec as P


def layer_norm(stream, norm_gain):
    widened = stream.astype(jnp.float32)
    row_mean = jnp.mean(widened, axis=-1, keepdims=True)
    variance = jnp.mean(jnp.square(widened - row_mean), axis=-1, keepdims=True)
    return ((widened - row_mean) * lax.rsqrt(variance + 1e-05) * norm_gain).astype(jnp.bfloat16)


def shared_branch(normed, shared_gate, shared_up, shared_down):
    shared_hidden = (
        jax.nn.silu(jnp.dot(normed, shared_gate, preferred_element_type=jnp.float32))
        * jnp.dot(normed, shared_up, preferred_element_type=jnp.float32)
    ).astype(jnp.bfloat16)
    return jnp.dot(shared_hidden, shared_down, preferred_element_type=jnp.float32)


def serve_rows(received, w_gate, w_up, w_down):
    local_count = w_gate.shape[0]
    blocks = received.reshape((-1, local_count) + received.shape[1:])
    gate_act = jnp.einsum("sxcd,xdh->sxch", blocks, w_gate, preferred_element_type=jnp.float32)
    up_act = jnp.einsum("sxcd,xdh->sxch", blocks, w_up, preferred_element_type=jnp.float32)
    hidden = (jax.nn.silu(gate_act) * up_act).astype(jnp.bfloat16)
    produced = jnp.einsum(
        "sxch,xhd->sxcd", hidden, w_down, preferred_element_type=jnp.float32
    ).astype(jnp.bfloat16)
    return lax.all_to_all(
        produced.reshape(received.shape), "ep", split_axis=0, concat_axis=0, tiled=True
    )


def generic_device(
    stream, norm_gain, routing, gates, w_gate, w_up, w_down, shared_gate, shared_up, shared_down
):
    tok_rows, top_count = routing.shape
    local_count = w_gate.shape[0]
    peer_count = lax.axis_size("ep")
    experts = local_count * peer_count
    capacity = 2 * tok_rows * top_count // experts
    normed = layer_norm(stream, norm_gain)
    row_ids = jnp.arange(tok_rows, dtype=jnp.int32)
    lower = (row_ids[:, None] > row_ids[None, :]).astype(jnp.bfloat16)
    slot_ids = jnp.arange(capacity, dtype=jnp.int32).astype(jnp.float32)
    expert_hits = (
        routing[:, :, None] == jnp.arange(experts, dtype=jnp.int32)[None, None, :]
    ).astype(jnp.float32)
    token_hits = jnp.sum(expert_hits, axis=1).astype(jnp.bfloat16)
    earlier = jnp.dot(lower, token_hits, preferred_element_type=jnp.float32)
    slot_index = jnp.sum(earlier[:, None, :] * expert_hits, axis=2)
    slot_hits = (slot_index[:, :, None] == slot_ids[None, None, :]).astype(jnp.float32)
    gate_table = jnp.sum(
        gates[:, :, None, None] * expert_hits[:, :, :, None] * slot_hits[:, :, None, :], axis=1
    )
    all_normed = lax.all_gather(normed, "ep", axis=0, tiled=True)
    all_routing = lax.all_gather(routing, "ep", axis=0, tiled=True)
    first_expert = lax.axis_index("ep") * local_count
    shifted = all_routing.reshape(peer_count, tok_rows, top_count) - first_expert
    local_hits = (
        shifted[:, :, :, None] == jnp.arange(local_count, dtype=jnp.int32)[None, None, None, :]
    ).astype(jnp.float32)
    hits_here = jnp.sum(local_hits, axis=2).astype(jnp.bfloat16)
    prior_here = jnp.einsum("ab,pbx->pax", lower, hits_here, preferred_element_type=jnp.float32)
    placing_here = (
        hits_here.astype(jnp.float32)[:, :, :, None]
        * (prior_here[:, :, :, None] == slot_ids[None, None, None, :]).astype(jnp.float32)
    ).astype(jnp.bfloat16)
    sources = all_normed.reshape(peer_count, tok_rows, all_normed.shape[1])
    incoming = jnp.einsum(
        "ptxc,ptd->pxcd", placing_here, sources, preferred_element_type=jnp.float32
    ).astype(jnp.bfloat16)
    returned = serve_rows(
        incoming.reshape(peer_count * local_count, capacity, all_normed.shape[1]),
        w_gate,
        w_up,
        w_down,
    )
    weight_high = gate_table.astype(jnp.bfloat16)
    weight_low = (gate_table - weight_high.astype(jnp.float32)).astype(jnp.bfloat16)
    routed = jnp.einsum("tec,ecd->td", weight_high, returned, preferred_element_type=jnp.float32)
    routed = routed + jnp.einsum(
        "tec,ecd->td", weight_low, returned, preferred_element_type=jnp.float32
    )
    shared = shared_branch(normed, shared_gate, shared_up, shared_down)
    return (routed + shared).astype(jnp.bfloat16)


CORNER = (
    1104, 1102, 1201, 2000, 1103, 1203, 1204, 1105, 1207, 1125, 1126, 1206, 1215, 1200, 1123, 1202,
    1120, 1121, 1212, 1205, 1122, 1106, 1101, 2020, 3020, 2030, 1161, 1216, 1230, 1163, 3030, 1162,
    4227, 1160, 4237, 4234, 4133, 4224, 4132, 3000, 4136, 4131, 4223, 1107, 2070, 1100, 4222, 4226,
    3070, 4221, 4135, 4277, 4170, 4171, 2060, 4172, 4275, 4276, 1143, 3060, 2010, 4274, 1147, 4260,
    1146, 4262, 4261, 3010, 4173, 1155, 1154, 4264, 4266, 2050, 4113, 4265, 4263, 4114, 4267, 3050,
    2040, 4252, 4110, 4251, 4153, 4157, 3040, 4250, 4145, 4156, 4241, 4144, 4243, 4242, 4255, 4111,
    4116, 4254, 4246, 4115, 4247, 4117, 4130, 4112, 4240, 5004, 4225, 5003, 5001, 5000, 5006, 4220,
    5007, 5005, 5002,
)
MIDDLE = (
    1023, 1025, 1321, 1424, 1323, 1427, 1425, 1324, 1026, 1021, 1020, 1420, 1326, 1401, 1327, 1403,
    1404, 1027, 1407, 1022, 1024, 1303, 2020, 1406, 1340, 1361, 1037, 1034, 1325, 1402, 1322, 1061,
    1400, 1367, 1364, 1063, 1422, 1415, 1405, 1300, 1362, 1062, 1366, 1421, 3020, 1307, 1423, 1363,
    1060, 1435, 2000, 1074, 1077, 1426, 2030, 1410, 2060, 1075, 1076, 1065, 1431, 1067, 1347, 1064,
    1434, 1066, 1433, 1301, 1043, 1304, 1342, 3030, 3060, 1046, 2070, 1047, 2040, 3000, 4337, 3040,
    1346, 3070, 1050, 1054, 4373, 1055, 4371, 4372, 1052, 4470, 4445, 4444, 2050, 4336, 1051, 1041,
    4377, 2010, 4475, 1040, 3050, 1042, 4460, 3010, 4030, 4374, 4453, 4462, 4314, 4376, 4464, 4461,
    4015, 4317, 4313, 4466, 4310, 4311, 4004, 4463, 4332, 4002, 4467, 4012, 4451, 4352, 4357, 4016,
    4006, 4003, 4465, 4441, 4001, 4333, 4443, 4000, 4442, 4007, 4356, 4455, 4331, 4350, 4454, 4446,
    4335, 4005, 5021, 4447, 4334, 5022, 4440, 5023, 5024, 5025, 5027, 5026, 5020,
)
PARTS = 8


def step_of(code):
    kind, to, block, part = "gxsrf"[code // 1000 - 1], "ABCDE"[code // 100 % 10], chr(65 + code // 10 % 10), str(code % 10)
    return kind + (to if kind in "gr" else "") + block + (part if kind in "grf" else "")


PLANS = {"A": [step_of(code) for code in CORNER], "C": [step_of(code) for code in MIDDLE]}


def across(block):
    return chr(65 + ((ord(block) - 65) ^ 1))


def ahead(block):
    n = ord(block) - 65
    return chr(65 + (3 - n // 2) * 2 + n % 2)


def seen_from(role, to, block):
    if to in ("A", "C"):
        return to, block
    if to in ("B", "D"):
        return role, across(block)
    return role, ahead(block)


SLOT = {role: {s[1]: i for i, s in enumerate([s for s in plan if s[0] == "s"])} for role, plan in PLANS.items()}
LANDING = {"A": {}, "C": {}}
for _role, _plan in PLANS.items():
    for _step in _plan:
        if _step[0] == "r":
            _there, _name = seen_from(_role, _step[1], _step[2])
            LANDING[_there][(_name, _step[3], _role, _step[1])] = len(LANDING[_there])
LANDINGS = max(len(v) for v in LANDING.values())
SENDS = 24 + max(sum(2 if s[0] == "g" else 1 for s in plan) for plan in PLANS.values())
R_META, R_SIB, R_SIBMETA, R_PAIR, R_LAND = 8 * PARTS, 8 * PARTS + 8, 8 * PARTS + 16, 8 * PARTS + 24, 8 * PARTS + 32


def fused_kernel(
    sizes, stream_hbm, gain, routing, gates, wg_hbm, wu_hbm, wd_hbm, sg_hbm, su_hbm, sd_hbm, out,
    tok0, tok1, mine, meta, pair_in, flow_in, wg, wu, wd, inc, slot_gate, place, shared,
    stream, send_sem, recv_sem, load_sem,
):
    n, local_count, capacity, top = sizes
    rows, width = stream.shape
    part_rows = rows // PARTS
    me = lax.axis_index("ep")
    z, y, core = me // 4, (me // 2) % 2, me % 2
    z_next = z + 1 - 2 * (z % 2)
    is_corner = z * (3 - z) == 0
    peers = {
        "A": z_next * 4 + y * 2 + core,
        "C": z_next * 4 + y * 2 + core,
        "B": z * 4 + (1 - y) * 2 + core,
        "D": z * 4 + (1 - y) * 2 + core,
        "E": (3 - z) * 4 + y * 2 + core,
    }
    sibling = z * 4 + y * 2 + 1 - core

    def when_role(role):
        return pl.when(is_corner if role == "A" else jnp.logical_not(is_corner))

    barrier = pltpu.get_barrier_semaphore()

    def greet(who):
        pl.semaphore_signal(
            barrier, inc=1, device_id={"ep": who}, device_id_type=pl.DeviceIdType.MESH
        )

    greet(sibling)
    greet(peers["A"])
    greet(peers["B"])

    @when_role("C")
    def _():
        greet(peers["E"])

    rows_in = [
        pltpu.make_async_copy(
            stream_hbm.at[pl.ds(p * part_rows, part_rows)], stream.at[pl.ds(p * part_rows, part_rows)],
            load_sem.at[9 + p],
        )
        for p in range(PARTS)
    ]
    for copy in rows_in:
        copy.start()
    loads = [
        pltpu.make_async_copy(src, dst, load_sem.at[i])
        for i, (src, dst) in enumerate(
            [
                (sg_hbm, wg.at[1]), (su_hbm, wu.at[1]), (sd_hbm, wd.at[1]),
                (wg_hbm.at[0], wg.at[0]), (wu_hbm.at[0], wu.at[0]), (wd_hbm.at[0], wd.at[0]),
                (wg_hbm.at[1], wg.at[1]), (wu_hbm.at[1], wu.at[1]), (wd_hbm.at[1], wd.at[1]),
            ]
        )
    ]
    for load in loads[:6]:
        load.start()

    def remote(src, dst, send, recv, peer):
        return pltpu.make_async_remote_copy(
            src_ref=src, dst_ref=dst, send_sem=send_sem.at[send], recv_sem=recv_sem.at[recv],
            device_id={"ep": peer}, device_id_type=pl.DeviceIdType.MESH,
        )

    def span_of(part):
        return pl.ds(int(part) * part_rows, part_rows)

    def sibling_copies(slot):
        return (
            remote(meta.at[slot, 0], meta.at[slot, 1], slot, R_SIBMETA + slot, sibling),
            remote(tok0.at[slot], tok1.at[slot], 8 + slot, R_SIB + slot, sibling),
        )

    def pair_copy(slot):
        return remote(tok1.at[slot], pair_in.at[slot], 16 + slot, R_PAIR + slot, sibling)

    piece = 16

    def add_rows(dst, begin, count, others, onto=None):
        def step(i, carry):
            offset = pl.multiple_of(i * piece, piece)
            span = pl.ds(begin + offset, piece)
            total = dst[span, :].astype(jnp.float32)
            for other, start in others:
                total = total + other[pl.ds(start + offset, piece), :].astype(jnp.float32)
            if onto is None:
                dst[span, :] = total.astype(jnp.bfloat16)
            else:
                out[span, :] = (total + onto[span, :]).astype(jnp.bfloat16)
            return carry

        lax.fori_loop(0, count // piece, step, 0)

    class Walk:
        def __init__(self, role):
            self.role, self.own, self.slots = role, role, SLOT[role]
            self.waited, self.used, self.copies = set(), 24, []

        def arrived(self, src, recv, key):
            if key not in self.waited:
                self.waited.add(key)
                remote(src, src, 0, recv, sibling).wait_recv()

        def tokens(self, block, part):
            slot = self.slots[block]
            if block != self.own:
                self.arrived(tok0.at[slot, span_of(part)], slot * PARTS + int(part), ("t", block, part))

        def details(self, block):
            slot = self.slots[block]
            if block != self.own:
                self.arrived(meta.at[slot, 0], R_META + slot, ("m", block))

        def push(self, views, recv, to):
            send, self.used = self.used, self.used + 1

            def copy():
                src, dst = views()
                return remote(src, dst, send, recv, peers[to])

            self.copies.append(copy)
            copy().start()

        def summed(self, block, part, last=False):
            slot, span = self.slots[block], span_of(part)
            others = []
            self.arrived(pair_in.at[slot], R_PAIR + slot, ("p", block))
            others.append((pair_in.at[slot], int(part) * part_rows))
            for (name, which, _, _), k in LANDING[self.role].items():
                if (name, which) == (block, part):
                    self.arrived(flow_in.at[k], R_LAND + k, ("l", k))
                    others.append((flow_in.at[k], 0))
            add_rows(mine.at[slot], int(part) * part_rows, part_rows, others, shared if last else None)

        def run(self, step):
            if step[0] == "g":
                to, block, part = step[1:]
                there, name = seen_from(self.role, to, block)
                slot, target = self.slots[block], SLOT[there][name]
                if part == "0":
                    self.details(block)
                    self.push(lambda: (meta.at[slot, 0], meta.at[target, 0]), R_META + target, to)
                self.tokens(block, part)
                self.push(
                    lambda: (tok0.at[slot, span_of(part)], tok0.at[target, span_of(part)]),
                    target * PARTS + int(part), to,
                )
            elif step[0] == "x":
                block = step[1]
                self.details(block)
                for part in range(PARTS):
                    self.tokens(block, str(part))
                for copy in sibling_copies(self.slots[block]):
                    copy.start()
            elif step[0] == "r":
                to, block, part = step[1:]
                there, name = seen_from(self.role, to, block)
                self.summed(block, part)
                k = LANDING[there][(name, part, self.role, to)]
                slot = self.slots[block]
                self.push(lambda: (mine.at[slot, span_of(part)], flow_in.at[k]), R_LAND + k, to)
            elif step[0] == "f":
                self.summed(step[1], step[2], last=True)

    walks = {role: Walk(role) for role in PLANS}
    segments = {}
    for role, plan in PLANS.items():
        parts = [[]]
        for step in plan:
            if step[0] == "s":
                parts.append([])
            else:
                parts[-1].append(step)
        mark = 0
        while mark < len(parts[0]) and parts[0][mark].rstrip("01234567")[-1] == role and parts[0][mark][0] in "gx":
            mark += 1
        segments[role] = [parts[0][:mark], parts[0][mark:]] + parts[1:]

    def run_segment(role, i):
        for step in segments[role][i]:
            walks[role].run(step)

    def norm_part(slot, part):
        span = pl.ds(pl.multiple_of(part * part_rows, part_rows), part_rows)
        wide = stream[span, :].astype(jnp.float32)
        mean = jnp.mean(wide, axis=-1, keepdims=True)
        centred = wide - mean
        var = jnp.mean(centred * centred, axis=-1, keepdims=True)
        tok0[slot, span, :] = (centred * lax.rsqrt(var + 1e-05) * gain[...]).astype(jnp.bfloat16)

    own_slot = lax.select(is_corner, SLOT["A"]["A"], SLOT["C"]["C"])
    meta[own_slot, 0, 0:top] = routing[...].astype(jnp.float32)
    meta[own_slot, 0, top:2 * top] = gates[...]

    def begin(role, neighbours):
        own = SLOT[role][role]
        steps = sorted(segments[role][0], key=lambda s: s[0] == "x")
        order = list(dict.fromkeys(int(s[3]) for s in steps if s[0] == "g"))[:2]
        ready = 0
        for step in steps:
            need = 3 if step[0] == "x" or int(step[3]) not in order else order.index(int(step[3])) + 1
            while ready < need:
                if ready < len(order):
                    rows_in[order[ready]].wait()
                    norm_part(own, order[ready])
                    if ready == 0:
                        pl.semaphore_wait(barrier, neighbours)
                elif ready == 2:
                    for p in range(PARTS):
                        if p not in order:
                            rows_in[p].wait()

                    def norm_rest(p, carry):
                        @pl.when((p != order[0]) & (p != order[1]))
                        def _():
                            norm_part(own, p)

                        return carry

                    lax.fori_loop(0, PARTS, norm_rest, 0)
                ready += 1
            walks[role].run(step)
        assert ready == 3

    @when_role("A")
    def _():
        begin("A", 3)

    @when_role("C")
    def _():
        begin("C", 4)

    def hidden_of(x, slot):
        gate = jnp.dot(x, wg[slot], preferred_element_type=jnp.float32)
        up = jnp.dot(x, wu[slot], preferred_element_type=jnp.float32)
        return jax.nn.silu(gate) * up

    cols = width // 4

    for load in loads[:3]:
        load.wait()
    hidden = hidden_of(tok0[own_slot], 1).astype(jnp.bfloat16)
    for c in range(4):
        part = pl.ds(c * cols, cols)
        shared[:, part] = jnp.dot(hidden, wd[1, :, part], preferred_element_type=jnp.float32)
    for load in loads[6:]:
        load.start()

    first = (me * local_count).astype(jnp.float32)
    tri = (
        lax.broadcasted_iota(jnp.int32, (rows, rows), 0)
        < lax.broadcasted_iota(jnp.int32, (rows, rows), 1)
    ).astype(jnp.float32).astype(jnp.bfloat16)
    slots = local_count * capacity
    slot_row = lax.broadcasted_iota(jnp.int32, (slots, rows), 0).astype(jnp.float32)
    stack_row = lax.broadcasted_iota(jnp.int32, (8, rows), 0)

    def serve(g):
        stacked = jnp.zeros((8, rows), jnp.float32)
        gate_rows, hit_rows = [], []
        for r in range(2):
            m = meta[g, r]
            ids, weights = m[0:top], m[top:2 * top]
            for x in range(local_count):
                match = (ids == first + x).astype(jnp.float32)
                hit = jnp.sum(match, axis=0, keepdims=True)
                hit_rows.append(hit)
                gate_rows.append(jnp.sum(match * weights, axis=0, keepdims=True))
                stacked = jnp.where(stack_row == r * local_count + x, hit, stacked)
        prior = jnp.dot(stacked.astype(jnp.bfloat16), tri, preferred_element_type=jnp.float32)
        for r in range(2):
            chosen = jnp.zeros((slots, rows), jnp.float32)
            weighted = jnp.zeros((slots, rows), jnp.float32)
            for x in range(local_count):
                q = r * local_count + x
                row = jnp.where(hit_rows[q] > 0, prior[q:q + 1] + x * capacity, -1.0)
                same = (slot_row == row).astype(jnp.float32)
                chosen = chosen + same
                weighted = weighted + same * gate_rows[q]
            slot_gate[r] = jnp.broadcast_to(jnp.sum(weighted, axis=1, keepdims=True), (slots, 128))
            place[r] = chosen.astype(jnp.bfloat16)
            source = tok0 if r == 0 else tok1
            for c in range(4):
                part = pl.ds(c * cols, cols)
                inc[r, :, part] = jnp.dot(
                    place[r], source[g, :, part], preferred_element_type=jnp.float32
                ).astype(jnp.bfloat16)
        for x in range(local_count):
            held = pl.ds(x * capacity, capacity)
            taken = inc[:, held, :].reshape(2 * capacity, width)
            scale = slot_gate[:, held, :].reshape(2 * capacity, 128)[:, 0:1]
            act = (hidden_of(taken, x) * scale).astype(jnp.bfloat16)
            for c in range(4):
                part = pl.ds(c * cols, cols)
                made = jnp.dot(act, wd[x, :, part], preferred_element_type=jnp.float32)
                inc[:, held, part] = made.astype(jnp.bfloat16).reshape(2, capacity, cols)
        for r in (1, 0):
            for c in range(4):
                part = pl.ds(c * cols, cols)
                total = lax.dot_general(
                    place[r], inc[r, :, part], (((0,), (0,)), ((), ())),
                    preferred_element_type=jnp.float32,
                ).astype(jnp.bfloat16)
                if r == 0:
                    mine[g, :, part] = total
                else:
                    tok1[g, :, part] = total
            if r == 1:
                pair_copy(g).start()

    def block(g, carry):
        for i in range(8):
            for role in PLANS:
                @pl.when((g == i) & (is_corner if role == "A" else jnp.logical_not(is_corner)))
                def _():
                    run_segment(role, i + 1)

        @pl.when(g == 0)
        def _():
            for load in loads[3:]:
                load.wait()

        for copy in sibling_copies(g):
            copy.wait_recv()
        serve(g)
        return carry

    lax.fori_loop(0, 8, block, 0)

    for role in PLANS:
        @when_role(role)
        def _():
            run_segment(role, 9)
            for copy in walks[role].copies:
                copy().wait_send()

    def drain(g, carry):
        for copy in sibling_copies(g) + (pair_copy(g),):
            copy.wait_send()
        return carry

    lax.fori_loop(0, 8, drain, 0)


def fused_device(
    stream, norm_gain, routing, gates, w_gate, w_up, w_down, shared_gate, shared_up, shared_down
):
    rows, width = stream.shape
    top = routing.shape[1]
    local_count, _, hidden = w_gate.shape
    n = lax.axis_size("ep")
    capacity = 2 * rows * top // (local_count * n)
    slots = local_count * capacity
    bf16, f32 = jnp.bfloat16, jnp.float32
    vmem, anywhere = pl.BlockSpec(memory_space=pltpu.VMEM), pl.BlockSpec(memory_space=pl.ANY)
    return pl.pallas_call(
        functools.partial(fused_kernel, (n, local_count, capacity, top)),
        out_shape=pltpu.VMEM((rows, width), bf16),
        in_specs=[anywhere] + [vmem] * 3 + [anywhere] * 6,
        out_specs=vmem,
        scratch_shapes=[
            pltpu.VMEM((8, rows, width), bf16),
            pltpu.VMEM((8, rows, width), bf16),
            pltpu.VMEM((8, rows, width), bf16),
            pltpu.VMEM((8, 2, 2 * top, rows), f32),
            pltpu.VMEM((8, rows, width), bf16),
            pltpu.VMEM((LANDINGS, rows // PARTS, width), bf16),
            pltpu.VMEM((2, width, hidden), bf16),
            pltpu.VMEM((2, width, hidden), bf16),
            pltpu.VMEM((2, hidden, width), bf16),
            pltpu.VMEM((2, slots, width), bf16),
            pltpu.VMEM((2, slots, 128), f32),
            pltpu.VMEM((2, slots, rows), bf16),
            pltpu.VMEM((rows, width), f32),
            pltpu.VMEM((rows, width), bf16),
            pltpu.SemaphoreType.DMA((SENDS,)),
            pltpu.SemaphoreType.DMA((R_LAND + LANDINGS,)),
            pltpu.SemaphoreType.DMA((9 + PARTS,)),
        ],
        compiler_params=pltpu.CompilerParams(
            collective_id=0, has_side_effects=True, vmem_limit_bytes=61 * 1024 * 1024
        ),
    )(
        stream, norm_gain.reshape(1, -1), routing.T, gates.T,
        w_gate, w_up, w_down, shared_gate, shared_up, shared_down,
    )


def on_device(stream, norm_gain, routing, gates, w_gate, *rest):
    ring = lax.axis_size("ep") // 4
    fits = ring == 4 and w_gate.shape[0] == 2 and rest[2].shape == w_gate.shape[1:]
    run = fused_device if fits else generic_device
    return run(stream, norm_gain, routing, gates, w_gate, *rest)


def solution(mesh):
    placed = (
        P(("grp", "ep"), None),
        P(),
        P(("grp", "ep"), None),
        P(("grp", "ep"), None),
        P("ep", None, None),
        P("ep", None, None),
        P("ep", None, None),
        P(),
        P(),
        P(),
    )
    return jax.shard_map(
        on_device, mesh=mesh, in_specs=placed, out_specs=P(("grp", "ep"), None), check_vma=False
    )
```

```python
import functools
import jax
import jax.numpy as jnp
from jax import lax
from jax.experimental import pallas as pl
from jax.experimental.pallas import tpu as pltpu
from jax.sharding import PartitionSpec as P


def layer_norm(stream, norm_gain):
    widened = stream.astype(jnp.float32)
    row_mean = jnp.mean(widened, axis=-1, keepdims=True)
    variance = jnp.mean(jnp.square(widened - row_mean), axis=-1, keepdims=True)
    return ((widened - row_mean) * lax.rsqrt(variance + 1e-05) * norm_gain).astype(jnp.bfloat16)


def shared_branch(normed, shared_gate, shared_up, shared_down):
    shared_hidden = (
        jax.nn.silu(jnp.dot(normed, shared_gate, preferred_element_type=jnp.float32))
        * jnp.dot(normed, shared_up, preferred_element_type=jnp.float32)
    ).astype(jnp.bfloat16)
    return jnp.dot(shared_hidden, shared_down, preferred_element_type=jnp.float32)


def serve_rows(received, w_gate, w_up, w_down):
    local_count = w_gate.shape[0]
    blocks = received.reshape((-1, local_count) + received.shape[1:])
    gate_act = jnp.einsum("sxcd,xdh->sxch", blocks, w_gate, preferred_element_type=jnp.float32)
    up_act = jnp.einsum("sxcd,xdh->sxch", blocks, w_up, preferred_element_type=jnp.float32)
    hidden = (jax.nn.silu(gate_act) * up_act).astype(jnp.bfloat16)
    produced = jnp.einsum(
        "sxch,xhd->sxcd", hidden, w_down, preferred_element_type=jnp.float32
    ).astype(jnp.bfloat16)
    return lax.all_to_all(
        produced.reshape(received.shape), "ep", split_axis=0, concat_axis=0, tiled=True
    )


def generic_device(
    stream, norm_gain, routing, gates, w_gate, w_up, w_down, shared_gate, shared_up, shared_down
):
    tok_rows, top_count = routing.shape
    local_count = w_gate.shape[0]
    peer_count = lax.axis_size("ep")
    experts = local_count * peer_count
    capacity = 2 * tok_rows * top_count // experts
    normed = layer_norm(stream, norm_gain)
    row_ids = jnp.arange(tok_rows, dtype=jnp.int32)
    lower = (row_ids[:, None] > row_ids[None, :]).astype(jnp.bfloat16)
    slot_ids = jnp.arange(capacity, dtype=jnp.int32).astype(jnp.float32)
    expert_hits = (
        routing[:, :, None] == jnp.arange(experts, dtype=jnp.int32)[None, None, :]
    ).astype(jnp.float32)
    token_hits = jnp.sum(expert_hits, axis=1).astype(jnp.bfloat16)
    earlier = jnp.dot(lower, token_hits, preferred_element_type=jnp.float32)
    slot_index = jnp.sum(earlier[:, None, :] * expert_hits, axis=2)
    slot_hits = (slot_index[:, :, None] == slot_ids[None, None, :]).astype(jnp.float32)
    gate_table = jnp.sum(
        gates[:, :, None, None] * expert_hits[:, :, :, None] * slot_hits[:, :, None, :], axis=1
    )
    all_normed = lax.all_gather(normed, "ep", axis=0, tiled=True)
    all_routing = lax.all_gather(routing, "ep", axis=0, tiled=True)
    first_expert = lax.axis_index("ep") * local_count
    shifted = all_routing.reshape(peer_count, tok_rows, top_count) - first_expert
    local_hits = (
        shifted[:, :, :, None] == jnp.arange(local_count, dtype=jnp.int32)[None, None, None, :]
    ).astype(jnp.float32)
    hits_here = jnp.sum(local_hits, axis=2).astype(jnp.bfloat16)
    prior_here = jnp.einsum("ab,pbx->pax", lower, hits_here, preferred_element_type=jnp.float32)
    placing_here = (
        hits_here.astype(jnp.float32)[:, :, :, None]
        * (prior_here[:, :, :, None] == slot_ids[None, None, None, :]).astype(jnp.float32)
    ).astype(jnp.bfloat16)
    sources = all_normed.reshape(peer_count, tok_rows, all_normed.shape[1])
    incoming = jnp.einsum(
        "ptxc,ptd->pxcd", placing_here, sources, preferred_element_type=jnp.float32
    ).astype(jnp.bfloat16)
    returned = serve_rows(
        incoming.reshape(peer_count * local_count, capacity, all_normed.shape[1]),
        w_gate,
        w_up,
        w_down,
    )
    weight_high = gate_table.astype(jnp.bfloat16)
    weight_low = (gate_table - weight_high.astype(jnp.float32)).astype(jnp.bfloat16)
    routed = jnp.einsum("tec,ecd->td", weight_high, returned, preferred_element_type=jnp.float32)
    routed = routed + jnp.einsum(
        "tec,ecd->td", weight_low, returned, preferred_element_type=jnp.float32
    )
    shared = shared_branch(normed, shared_gate, shared_up, shared_down)
    return (routed + shared).astype(jnp.bfloat16)


CORNER = (
    1104, 1102, 1201, 2000, 1103, 1203, 1204, 1105, 1207, 1125, 1126, 1206, 1215, 1200, 1123, 1202,
    1120, 1121, 1212, 1205, 1122, 1106, 1101, 2020, 3020, 2030, 1161, 1216, 1230, 1163, 3030, 1162,
    4227, 1160, 4237, 4234, 4133, 4224, 4132, 3000, 4136, 4131, 4223, 1107, 2070, 1100, 4222, 4226,
    3070, 4221, 4135, 4277, 4170, 4171, 2060, 4172, 4275, 4276, 1143, 3060, 2010, 4274, 1147, 4260,
    1146, 4262, 4261, 3010, 4173, 1155, 1154, 4264, 4266, 2050, 4113, 4265, 4263, 4114, 4267, 3050,
    2040, 4252, 4110, 4251, 4153, 4157, 3040, 4250, 4145, 4156, 4241, 4144, 4243, 4242, 4255, 4111,
    4116, 4254, 4246, 4115, 4247, 4117, 4130, 4112, 4240, 5004, 4225, 5000, 5003, 5001, 5006, 4220,
    5007, 5005, 5002,
)
MIDDLE = (
    1023, 1025, 1321, 1424, 1323, 1427, 1425, 1324, 1026, 1021, 1020, 1420, 1326, 1401, 1327, 1403,
    1404, 1027, 1407, 1022, 1024, 1303, 2020, 1406, 1340, 1361, 1037, 1034, 1325, 1402, 1322, 1061,
    1400, 1367, 1364, 1063, 1422, 1415, 1405, 1300, 1362, 1062, 1366, 1421, 3020, 1307, 1423, 1363,
    1060, 1435, 2000, 1074, 1077, 1426, 2030, 1410, 2060, 1075, 1076, 1065, 1431, 1067, 1347, 1064,
    1434, 1433, 1066, 1301, 1043, 1304, 1342, 3030, 3060, 1046, 2070, 1047, 2040, 3000, 4337, 3040,
    1346, 3070, 1050, 1054, 4373, 1055, 4371, 4372, 1052, 4470, 4445, 4444, 2050, 4336, 1051, 1041,
    4377, 2010, 4475, 1040, 3050, 1042, 4460, 3010, 4030, 4374, 4453, 4462, 4314, 4376, 4464, 4461,
    4015, 4317, 4313, 4466, 4310, 4311, 4004, 4463, 4332, 4002, 4467, 4012, 4451, 4352, 4357, 4016,
    4006, 4003, 4465, 4441, 4001, 4333, 4443, 4000, 4442, 4007, 4356, 4455, 4331, 4350, 4454, 4446,
    4335, 4005, 5021, 4447, 4334, 5022, 4440, 5023, 5024, 5025, 5027, 5026, 5020,
)
PARTS = 8


def step_of(code):
    kind, to, block, part = "gxsrf"[code // 1000 - 1], "ABCDE"[code // 100 % 10], chr(65 + code // 10 % 10), str(code % 10)
    return kind + (to if kind in "gr" else "") + block + (part if kind in "grf" else "")


PLANS = {"A": [step_of(code) for code in CORNER], "C": [step_of(code) for code in MIDDLE]}


def across(block):
    return chr(65 + ((ord(block) - 65) ^ 1))


def ahead(block):
    n = ord(block) - 65
    return chr(65 + (3 - n // 2) * 2 + n % 2)


def seen_from(role, to, block):
    if to in ("A", "C"):
        return to, block
    if to in ("B", "D"):
        return role, across(block)
    return role, ahead(block)


SLOT = {role: {s[1]: i for i, s in enumerate([s for s in plan if s[0] == "s"])} for role, plan in PLANS.items()}
LANDING = {"A": {}, "C": {}}
for _role, _plan in PLANS.items():
    for _step in _plan:
        if _step[0] == "r":
            _there, _name = seen_from(_role, _step[1], _step[2])
            LANDING[_there][(_name, _step[3], _role, _step[1])] = len(LANDING[_there])
LANDINGS = max(len(v) for v in LANDING.values())
SENDS = 24 + max(sum(2 if s[0] == "g" else 1 for s in plan) for plan in PLANS.values())
R_META, R_SIB, R_SIBMETA, R_PAIR, R_LAND = 8 * PARTS, 8 * PARTS + 8, 8 * PARTS + 16, 8 * PARTS + 24, 8 * PARTS + 32


def fused_kernel(
    sizes, stream_hbm, gain, routing, gates, wg_hbm, wu_hbm, wd_hbm, sg_hbm, su_hbm, sd_hbm, out,
    tok0, tok1, mine, meta, pair_in, flow_in, wg, wu, wd, inc, slot_gate, place, shared,
    stream, send_sem, recv_sem, load_sem,
):
    n, local_count, capacity, top = sizes
    rows, width = stream.shape
    part_rows = rows // PARTS
    me = lax.axis_index("ep")
    z, y, core = me // 4, (me // 2) % 2, me % 2
    z_next = z + 1 - 2 * (z % 2)
    is_corner = z * (3 - z) == 0
    peers = {
        "A": z_next * 4 + y * 2 + core,
        "C": z_next * 4 + y * 2 + core,
        "B": z * 4 + (1 - y) * 2 + core,
        "D": z * 4 + (1 - y) * 2 + core,
        "E": (3 - z) * 4 + y * 2 + core,
    }
    sibling = z * 4 + y * 2 + 1 - core

    def when_role(role):
        return pl.when(is_corner if role == "A" else jnp.logical_not(is_corner))

    barrier = pltpu.get_barrier_semaphore()

    def greet(who):
        pl.semaphore_signal(
            barrier, inc=1, device_id={"ep": who}, device_id_type=pl.DeviceIdType.MESH
        )

    greet(sibling)
    greet(peers["A"])
    greet(peers["B"])

    @when_role("C")
    def _():
        greet(peers["E"])

    rows_in = [
        pltpu.make_async_copy(
            stream_hbm.at[pl.ds(p * part_rows, part_rows)], stream.at[pl.ds(p * part_rows, part_rows)],
            load_sem.at[9 + p],
        )
        for p in range(PARTS)
    ]
    for copy in rows_in:
        copy.start()
    loads = [
        pltpu.make_async_copy(src, dst, load_sem.at[i])
        for i, (src, dst) in enumerate(
            [
                (sg_hbm, wg.at[1]), (su_hbm, wu.at[1]), (sd_hbm, wd.at[1]),
                (wg_hbm.at[0], wg.at[0]), (wu_hbm.at[0], wu.at[0]), (wd_hbm.at[0], wd.at[0]),
                (wg_hbm.at[1], wg.at[1]), (wu_hbm.at[1], wu.at[1]), (wd_hbm.at[1], wd.at[1]),
            ]
        )
    ]

    def remote(src, dst, send, recv, peer):
        return pltpu.make_async_remote_copy(
            src_ref=src, dst_ref=dst, send_sem=send_sem.at[send], recv_sem=recv_sem.at[recv],
            device_id={"ep": peer}, device_id_type=pl.DeviceIdType.MESH,
        )

    def span_of(part):
        return pl.ds(int(part) * part_rows, part_rows)

    def sibling_copies(slot):
        return (
            remote(meta.at[slot, 0], meta.at[slot, 1], slot, R_SIBMETA + slot, sibling),
            remote(tok0.at[slot], tok1.at[slot], 8 + slot, R_SIB + slot, sibling),
        )

    def pair_copy(slot):
        return remote(tok1.at[slot], pair_in.at[slot], 16 + slot, R_PAIR + slot, sibling)

    piece = 16

    def add_rows(dst, begin, count, others, onto=None):
        def step(i, carry):
            offset = pl.multiple_of(i * piece, piece)
            span = pl.ds(begin + offset, piece)
            total = dst[span, :].astype(jnp.float32)
            for other, start in others:
                total = total + other[pl.ds(start + offset, piece), :].astype(jnp.float32)
            if onto is None:
                dst[span, :] = total.astype(jnp.bfloat16)
            else:
                out[span, :] = (total + onto[span, :]).astype(jnp.bfloat16)
            return carry

        lax.fori_loop(0, count // piece, step, 0)

    class Walk:
        def __init__(self, role):
            self.role, self.own, self.slots = role, role, SLOT[role]
            self.waited, self.used, self.copies = set(), 24, []

        def arrived(self, src, recv, key):
            if key not in self.waited:
                self.waited.add(key)
                remote(src, src, 0, recv, sibling).wait_recv()

        def tokens(self, block, part):
            slot = self.slots[block]
            if block != self.own:
                self.arrived(tok0.at[slot, span_of(part)], slot * PARTS + int(part), ("t", block, part))

        def details(self, block):
            slot = self.slots[block]
            if block != self.own:
                self.arrived(meta.at[slot, 0], R_META + slot, ("m", block))

        def push(self, views, recv, to):
            send, self.used = self.used, self.used + 1

            def copy():
                src, dst = views()
                return remote(src, dst, send, recv, peers[to])

            self.copies.append(copy)
            copy().start()

        def summed(self, block, part, last=False):
            slot, span = self.slots[block], span_of(part)
            others = []
            self.arrived(pair_in.at[slot], R_PAIR + slot, ("p", block))
            others.append((pair_in.at[slot], int(part) * part_rows))
            for (name, which, _, _), k in LANDING[self.role].items():
                if (name, which) == (block, part):
                    self.arrived(flow_in.at[k], R_LAND + k, ("l", k))
                    others.append((flow_in.at[k], 0))
            add_rows(mine.at[slot], int(part) * part_rows, part_rows, others, shared if last else None)

        def run(self, step):
            if step[0] == "g":
                to, block, part = step[1:]
                there, name = seen_from(self.role, to, block)
                slot, target = self.slots[block], SLOT[there][name]
                if part == "0":
                    self.details(block)
                    self.push(lambda: (meta.at[slot, 0], meta.at[target, 0]), R_META + target, to)
                self.tokens(block, part)
                self.push(
                    lambda: (tok0.at[slot, span_of(part)], tok0.at[target, span_of(part)]),
                    target * PARTS + int(part), to,
                )
            elif step[0] == "x":
                block = step[1]
                self.details(block)
                for part in range(PARTS):
                    self.tokens(block, str(part))
                for copy in sibling_copies(self.slots[block]):
                    copy.start()
            elif step[0] == "r":
                to, block, part = step[1:]
                there, name = seen_from(self.role, to, block)
                self.summed(block, part)
                k = LANDING[there][(name, part, self.role, to)]
                slot = self.slots[block]
                self.push(lambda: (mine.at[slot, span_of(part)], flow_in.at[k]), R_LAND + k, to)
            elif step[0] == "f":
                self.summed(step[1], step[2], last=True)

    walks = {role: Walk(role) for role in PLANS}
    segments = {}
    for role, plan in PLANS.items():
        parts = [[]]
        for step in plan:
            if step[0] == "s":
                parts.append([])
            else:
                parts[-1].append(step)
        mark = 0
        while mark < len(parts[0]) and parts[0][mark].rstrip("01234567")[-1] == role and parts[0][mark][0] in "gx":
            mark += 1
        segments[role] = [parts[0][:mark], parts[0][mark:]] + parts[1:]

    def run_segment(role, i):
        for step in segments[role][i]:
            walks[role].run(step)

    def norm_part(slot, part):
        span = pl.ds(pl.multiple_of(part * part_rows, part_rows), part_rows)
        wide = stream[span, :].astype(jnp.float32)
        mean = jnp.mean(wide, axis=-1, keepdims=True)
        centred = wide - mean
        var = jnp.mean(centred * centred, axis=-1, keepdims=True)
        tok0[slot, span, :] = (centred * lax.rsqrt(var + 1e-05) * gain[...]).astype(jnp.bfloat16)

    own_slot = lax.select(is_corner, SLOT["A"]["A"], SLOT["C"]["C"])
    meta[own_slot, 0, 0:top] = routing[...].astype(jnp.float32)
    meta[own_slot, 0, top:2 * top] = gates[...]

    def begin(role, neighbours):
        own = SLOT[role][role]
        steps = sorted(segments[role][0], key=lambda s: s[0] == "x")
        order = list(dict.fromkeys(int(s[3]) for s in steps if s[0] == "g"))[:2]
        ready = 0
        for step in steps:
            need = 3 if step[0] == "x" or int(step[3]) not in order else order.index(int(step[3])) + 1
            while ready < need:
                if ready < len(order):
                    rows_in[order[ready]].wait()
                    norm_part(own, order[ready])
                    if ready == 0:
                        pl.semaphore_wait(barrier, neighbours)
                elif ready == 2:
                    for p in range(PARTS):
                        if p not in order:
                            rows_in[p].wait()

                    def norm_rest(p, carry):
                        @pl.when((p != order[0]) & (p != order[1]))
                        def _():
                            norm_part(own, p)

                        return carry

                    lax.fori_loop(0, PARTS, norm_rest, 0)
                ready += 1
            walks[role].run(step)
        assert ready == 3

    @when_role("A")
    def _():
        begin("A", 3)

    @when_role("C")
    def _():
        begin("C", 4)

    for load in loads[:6]:
        load.start()

    def hidden_of(x, slot):
        gate = jnp.dot(x, wg[slot], preferred_element_type=jnp.float32)
        up = jnp.dot(x, wu[slot], preferred_element_type=jnp.float32)
        return jax.nn.silu(gate) * up

    cols = width // 4

    for load in loads[:3]:
        load.wait()
    hidden = hidden_of(tok0[own_slot], 1).astype(jnp.bfloat16)
    for c in range(4):
        part = pl.ds(c * cols, cols)
        shared[:, part] = jnp.dot(hidden, wd[1, :, part], preferred_element_type=jnp.float32)
    for load in loads[6:]:
        load.start()

    first = (me * local_count).astype(jnp.float32)
    tri = (
        lax.broadcasted_iota(jnp.int32, (rows, rows), 0)
        < lax.broadcasted_iota(jnp.int32, (rows, rows), 1)
    ).astype(jnp.float32).astype(jnp.bfloat16)
    slots = local_count * capacity
    slot_row = lax.broadcasted_iota(jnp.int32, (slots, rows), 0).astype(jnp.float32)
    stack_row = lax.broadcasted_iota(jnp.int32, (8, rows), 0)

    def serve(g):
        stacked = jnp.zeros((8, rows), jnp.float32)
        gate_rows, hit_rows = [], []
        for r in range(2):
            m = meta[g, r]
            ids, weights = m[0:top], m[top:2 * top]
            for x in range(local_count):
                match = (ids == first + x).astype(jnp.float32)
                hit = jnp.sum(match, axis=0, keepdims=True)
                hit_rows.append(hit)
                gate_rows.append(jnp.sum(match * weights, axis=0, keepdims=True))
                stacked = jnp.where(stack_row == r * local_count + x, hit, stacked)
        prior = jnp.dot(stacked.astype(jnp.bfloat16), tri, preferred_element_type=jnp.float32)
        for r in range(2):
            chosen = jnp.zeros((slots, rows), jnp.float32)
            weighted = jnp.zeros((slots, rows), jnp.float32)
            for x in range(local_count):
                q = r * local_count + x
                row = jnp.where(hit_rows[q] > 0, prior[q:q + 1] + x * capacity, -1.0)
                same = (slot_row == row).astype(jnp.float32)
                chosen = chosen + same
                weighted = weighted + same * gate_rows[q]
            slot_gate[r] = jnp.broadcast_to(jnp.sum(weighted, axis=1, keepdims=True), (slots, 128))
            place[r] = chosen.astype(jnp.bfloat16)
            source = tok0 if r == 0 else tok1
            for c in range(4):
                part = pl.ds(c * cols, cols)
                inc[r, :, part] = jnp.dot(
                    place[r], source[g, :, part], preferred_element_type=jnp.float32
                ).astype(jnp.bfloat16)
        for x in range(local_count):
            held = pl.ds(x * capacity, capacity)
            taken = inc[:, held, :].reshape(2 * capacity, width)
            scale = slot_gate[:, held, :].reshape(2 * capacity, 128)[:, 0:1]
            act = (hidden_of(taken, x) * scale).astype(jnp.bfloat16)
            for c in range(4):
                part = pl.ds(c * cols, cols)
                made = jnp.dot(act, wd[x, :, part], preferred_element_type=jnp.float32)
                inc[:, held, part] = made.astype(jnp.bfloat16).reshape(2, capacity, cols)
        for r in (1, 0):
            for c in range(4):
                part = pl.ds(c * cols, cols)
                total = lax.dot_general(
                    place[r], inc[r, :, part], (((0,), (0,)), ((), ())),
                    preferred_element_type=jnp.float32,
                ).astype(jnp.bfloat16)
                if r == 0:
                    mine[g, :, part] = total
                else:
                    tok1[g, :, part] = total
            if r == 1:
                pair_copy(g).start()

    def block(g, carry):
        for i in range(8):
            for role in PLANS:
                @pl.when((g == i) & (is_corner if role == "A" else jnp.logical_not(is_corner)))
                def _():
                    run_segment(role, i + 1)

        @pl.when(g == 0)
        def _():
            for load in loads[3:]:
                load.wait()

        for copy in sibling_copies(g):
            copy.wait_recv()
        serve(g)
        return carry

    lax.fori_loop(0, 8, block, 0)

    def drain(g, carry):
        for copy in sibling_copies(g) + (pair_copy(g),):
            copy.wait_send()
        return carry

    for role in PLANS:
        @when_role(role)
        def _():
            walk, steps = walks[role], segments[role][9]
            for step in steps[:-4]:
                walk.run(step)
            old = len(walk.copies) - 24
            for copy in walk.copies[:old]:
                copy().wait_send()
            lax.fori_loop(0, 8, drain, 0)
            for step in steps[-4:]:
                walk.run(step)
            for copy in walk.copies[old:]:
                copy().wait_send()


def fused_device(
    stream, norm_gain, routing, gates, w_gate, w_up, w_down, shared_gate, shared_up, shared_down
):
    rows, width = stream.shape
    top = routing.shape[1]
    local_count, _, hidden = w_gate.shape
    n = lax.axis_size("ep")
    capacity = 2 * rows * top // (local_count * n)
    slots = local_count * capacity
    bf16, f32 = jnp.bfloat16, jnp.float32
    vmem, anywhere = pl.BlockSpec(memory_space=pltpu.VMEM), pl.BlockSpec(memory_space=pl.ANY)
    return pl.pallas_call(
        functools.partial(fused_kernel, (n, local_count, capacity, top)),
        out_shape=pltpu.VMEM((rows, width), bf16),
        in_specs=[anywhere] + [vmem] * 3 + [anywhere] * 6,
        out_specs=vmem,
        scratch_shapes=[
            pltpu.VMEM((8, rows, width), bf16),
            pltpu.VMEM((8, rows, width), bf16),
            pltpu.VMEM((8, rows, width), bf16),
            pltpu.VMEM((8, 2, 2 * top, rows), f32),
            pltpu.VMEM((8, rows, width), bf16),
            pltpu.VMEM((LANDINGS, rows // PARTS, width), bf16),
            pltpu.VMEM((2, width, hidden), bf16),
            pltpu.VMEM((2, width, hidden), bf16),
            pltpu.VMEM((2, hidden, width), bf16),
            pltpu.VMEM((2, slots, width), bf16),
            pltpu.VMEM((2, slots, 128), f32),
            pltpu.VMEM((2, slots, rows), bf16),
            pltpu.VMEM((rows, width), f32),
            pltpu.VMEM((rows, width), bf16),
            pltpu.SemaphoreType.DMA((SENDS,)),
            pltpu.SemaphoreType.DMA((R_LAND + LANDINGS,)),
            pltpu.SemaphoreType.DMA((9 + PARTS,)),
        ],
        compiler_params=pltpu.CompilerParams(
            collective_id=0, has_side_effects=True, vmem_limit_bytes=61 * 1024 * 1024
        ),
    )(
        stream, norm_gain.reshape(1, -1), routing.T, gates.T,
        w_gate, w_up, w_down, shared_gate, shared_up, shared_down,
    )


def on_device(stream, norm_gain, routing, gates, w_gate, *rest):
    ring = lax.axis_size("ep") // 4
    fits = ring == 4 and w_gate.shape[0] == 2 and rest[2].shape == w_gate.shape[1:]
    run = fused_device if fits else generic_device
    return run(stream, norm_gain, routing, gates, w_gate, *rest)


def solution(mesh):
    placed = (
        P(("grp", "ep"), None),
        P(),
        P(("grp", "ep"), None),
        P(("grp", "ep"), None),
        P("ep", None, None),
        P("ep", None, None),
        P("ep", None, None),
        P(),
        P(),
        P(),
    )
    return jax.shard_map(
        on_device, mesh=mesh, in_specs=placed, out_specs=P(("grp", "ep"), None), check_vma=False
    )
```
